1024 devices in a mesh: grp: 2 (over x), row: 16 (over z), col: 32 (over y, core).
Axes of the slice: x: 2, y: 16, z: 16, core: 2. Of those that a mesh axis runs over, the one named last changes fastest.
The devices are a block of a 4x16x16 slice.
Arguments:
- gate_in: bfloat16 [32, 4096, 1024], P(('grp', 'row'), 'col'), parts along dimension 0, may hold values from -6 to 6
- mult_in: bfloat16 [32, 4096, 1024], P(('grp', 'row'), 'col'), parts along dimension 0, may hold values from -6 to 6
- value_in: bfloat16 [32, 4096, 1024], P(('grp', 'row'), 'col'), parts along dimension 0, may hold values from -6 to 6
- taps_gate: float32 [3, 1024], replicated, may hold values from -3.5 to 3.5
- taps_mult: float32 [3, 1024], replicated, may hold values from -3.5 to 3.5
- taps_value: float32 [3, 1024], replicated, may hold values from -3.5 to 3.5
- filter_first: float32 [33, 128], replicated, may hold values from -3 to 3
- filter_second: float32 [128, 128], replicated, may hold values from -1 to 1
- filter_ahead: float32 [128, 1024], replicated, may hold values from -0.5 to 0.5
- filter_behind: float32 [128, 1024], replicated, may hold values from -0.5 to 0.5
- filter_decay: float32 [1024], replicated, may hold values from 0.05 to 136.5
- skip_gain: float32 [1024], replicated, may hold values from -5 to 5
- out_weight: bfloat16 [1024, 2048], replicated, may hold values from -0.1875 to 0.1875
Outputs:
- mixed: bfloat16 [32, 4096, 2048], P(('grp', 'row'), 'col'), parts along dimension 0
The draws below stay inside these ranges and needn't reach their ends.
There are 2 independent parts, one for each index of `grp`. The reference program is written for one: setup_inputs(seed, part) draws one part's arguments, and reference() takes and returns one part's arrays. A program takes and returns all parts, laid end to end along the dimension named above; an argument that names none is the same for every part. Nothing has to cross between parts.
All inputs are finite; a program needn't handle non-finite values.
Results may differ from the reference program's by a relative error of at most 0.0049.
Values may be sent and summed in bfloat16 or wider, within the bound.
No kernel may reach another device: no remote copies, remote signals or barrier semaphores. Data moves between devices by JAX's collectives and lax.ppermute only.
A program may use at most 32 MiB of HBM per device.

```python
import math
import jax
import jax.numpy as jnp
from jax import lax

D = 2048
H = 1024
FH = 128
FEAT = 33
TAPS = 3
SEQ = 4096
SEQS = 16


def draw_filter_decay(key, part):
    slow_key, fast_key, pick_key = jax.random.split(jax.random.fold_in(key, 7), 3)
    slow_rates = jnp.exp(jax.random.uniform(slow_key, (H,), jnp.float32, math.log(0.05), math.log(2.0)))
    fast_rates = (SEQ - 1) / jnp.exp(jax.random.uniform(fast_key, (H,), jnp.float32, math.log(30.0), math.log(100.0)))
    fast_share = 0.5
    chosen = jax.random.uniform(pick_key, (H,), jnp.float32) < fast_share
    return jnp.where(chosen, fast_rates, slow_rates)


def block_levels(key, shape, shards, low, high):
    level = 1.0
    for axis_at, parts in shards:
        heights = jax.random.uniform(jax.random.fold_in(jax.random.fold_in(key, 6), axis_at), (parts,), jnp.float32, low / len(shards), high / len(shards))
        level = level * jnp.repeat(jnp.exp(heights), shape[axis_at] // parts).reshape((-1,) + (1,) * (len(shape) - 1 - axis_at))
    return level


def gaussian(rng, extent, deviation, reach, cuts=(), kind=jnp.bfloat16):
    loudness = block_levels(rng, extent, cuts, -0.22, 0.18) if cuts else 1.0
    values = jax.random.normal(rng, extent, jnp.float32) * deviation * loudness
    return jnp.minimum(jnp.maximum(values, -reach), reach).astype(kind)


def setup_inputs(seed: int = 0, part: int = 0) -> dict:
    keys = jax.random.split(jax.random.key(seed), 14)
    own_keys = jax.random.split(jax.random.fold_in(keys[13], part), 14)
    return {
        "gate_in": gaussian(own_keys[0], (SEQS, SEQ, H), 1.0, 6.0, ((0, 16), (1, 32))),
        "mult_in": gaussian(own_keys[1], (SEQS, SEQ, H), 1.0, 6.0, ((0, 16), (1, 32))),
        "value_in": gaussian(own_keys[2], (SEQS, SEQ, H), 1.0, 6.0, ((0, 16), (1, 32))),
        "taps_gate": gaussian(keys[3], (TAPS, H), TAPS ** -0.5, 3.5, (), jnp.float32),
        "taps_mult": gaussian(keys[4], (TAPS, H), TAPS ** -0.5, 3.5, (), jnp.float32),
        "taps_value": gaussian(keys[5], (TAPS, H), TAPS ** -0.5, 3.5, (), jnp.float32),
        "filter_first": jnp.clip(jax.random.uniform(keys[6], (FEAT, FH), jnp.float32, -3.0, 3.0), -3.0, 3.0),
        "filter_second": jnp.clip(jax.random.uniform(keys[7], (FH, FH), jnp.float32, -1.0, 1.0), -1.0, 1.0),
        "filter_ahead": gaussian(keys[8], (FH, H), FH ** -0.5, 0.5, (), jnp.float32),
        "filter_behind": gaussian(keys[9], (FH, H), FH ** -0.5, 0.5, (), jnp.float32),
        "filter_decay": draw_filter_decay(jax.random.fold_in(keys[13], 71), part),
        "skip_gain": gaussian(keys[11], (H,), 1.0, 5.0, (), jnp.float32),
        "out_weight": gaussian(keys[12], (H, D), H ** -0.5, 0.1875),
    }


highest = lax.Precision.HIGHEST

def filter_hidden(mirror, seq_len, filter_first, filter_second):
    tau_values = mirror.astype(jnp.float32) / (seq_len - 1)
    omega_pos = 2.0 * math.pi / seq_len * mirror.astype(jnp.float32)
    band_count = (filter_first.shape[0] - 1) // 2
    band_values = jnp.linspace(0.0001, band_count - 1, band_count, dtype=jnp.float32)
    angles = omega_pos[:, None] * band_values[None, :]
    features = jnp.concatenate([tau_values[:, None], jnp.cos(angles), -jnp.sin(angles)], axis=1)
    hidden = jnp.sin(jnp.dot(features, filter_first, precision=highest))
    hidden = jnp.sin(jnp.dot(hidden, filter_second, precision=highest))
    return (hidden, tau_values)

def side_values(hidden, tau_values, side_weight, decay_rates):
    values = jnp.einsum('pf,fh->hp', hidden, side_weight, precision=highest)
    return values * jnp.exp(-decay_rates[:, None] * tau_values[None, :])

def short_conv(source, tap_weights):
    seq_len = source.shape[0]
    padded = jnp.pad(source.astype(jnp.float32), ((1, 1), (0, 0)))
    summed = jnp.zeros(source.shape, jnp.float32)
    for offset in range(tap_weights.shape[0]):
        summed = summed + tap_weights[offset] * padded[offset:offset + seq_len]
    return summed

def reference(gate_in, mult_in, value_in, taps_gate, taps_mult, taps_value, filter_first, filter_second, filter_ahead, filter_behind, filter_decay, skip_gain, out_weight):
    seq_len = gate_in.shape[1]
    span_len = 2 * seq_len
    mirror = jnp.arange(seq_len, dtype=jnp.int32)
    hidden, tau_values = filter_hidden(mirror, seq_len, filter_first, filter_second)
    ahead_vals = side_values(hidden, tau_values, filter_ahead, filter_decay)
    behind_vals = side_values(hidden, tau_values, filter_behind, filter_decay)
    kernel = jnp.concatenate([ahead_vals, jnp.zeros((ahead_vals.shape[0], 1), jnp.float32), jnp.flip(behind_vals[:, 1:], axis=1)], axis=1)
    kernel = kernel * lax.rsqrt(lax.optimization_barrier(jnp.sum(kernel * kernel, axis=1, keepdims=True)) + 1e-06)
    kernel_freq = jnp.fft.rfft(kernel, n=span_len, axis=1)

    def one_sequence(inputs):
        gate_rows, mult_rows, value_rows = inputs
        gate_part = short_conv(gate_rows, taps_gate)
        product = short_conv(value_rows, taps_value) * short_conv(mult_rows, taps_mult)
        spectrum = jnp.fft.rfft(product.T, n=span_len, axis=1)
        convolved = jnp.fft.irfft(spectrum * kernel_freq, n=span_len, axis=1)[:, :seq_len].T
        mixed_rows = ((convolved + skip_gain * product) * gate_part).astype(jnp.bfloat16)
        return jnp.dot(mixed_rows, out_weight, preferred_element_type=jnp.float32).astype(jnp.bfloat16)
    return lax.map(one_sequence, (gate_in, mult_in, value_in))
```

```python
import functools
import math

import jax
import jax.numpy as jnp
import numpy as np
from jax import lax
from jax.experimental import pallas as pl
from jax.experimental.pallas import tpu as pltpu
from jax.sharding import PartitionSpec as P

COL = "col"
F32 = jnp.float32
BF16 = jnp.bfloat16

TWO_PI_HEAD = np.float32(np.round(2.0 * math.pi * 2**14) / 2**14)
TWO_PI_TAIL = np.float32(2.0 * math.pi - float(TWO_PI_HEAD))


def sine_coefficients():
    nodes = np.cos((np.arange(4000) + 0.5) * math.pi / 8000) * math.pi * 1.0001
    basis = np.stack([nodes ** (2 * j + 1) for j in range(7)], axis=1)
    return [float(v) for v in np.linalg.lstsq(basis, np.sin(nodes), rcond=None)[0]]


SINE = sine_coefficients()


def sine(x):
    turns = jnp.floor(x * np.float32(0.5 / math.pi) + 0.5)
    r = (x - turns * TWO_PI_HEAD) - turns * TWO_PI_TAIL
    z = r * r
    total = np.float32(SINE[6]) * z + np.float32(SINE[5])
    for j in (4, 3, 2, 1, 0):
        total = total * z + np.float32(SINE[j])
    return total * r


def halves(x):
    high = x.astype(BF16)
    return high, (x - high.astype(F32)).astype(BF16)


def np_halves(x):
    high = np.asarray(x, np.float32).astype(BF16)
    return high, (np.asarray(x, np.float32) - high.astype(np.float32)).astype(BF16)


def dot(a, b):
    return jnp.dot(a, b, preferred_element_type=F32)


def tables(blocks, width):
    span = 2 * blocks * width
    freq = np.arange(blocks) + 0.5
    first = 2.0 * math.pi * np.outer(freq, np.arange(blocks)) / (2 * blocks)
    t1 = np.concatenate([np.cos(first), -np.sin(first)], axis=0)
    t3 = np.concatenate([np.cos(first).T, -np.sin(first).T], axis=1) * (2.0 / span)
    twist = 2.0 * math.pi * np.outer(freq, np.arange(width)) / span
    second = 2.0 * math.pi * (np.outer(np.arange(width), np.arange(width)) % width) / width
    c, s = np.cos(second), np.sin(second)
    ahead = np.block([[c, -s], [s, c]])
    back = np.block([[c, s], [-s, c]])
    mirror = ahead * np.where(np.arange(2 * width) < width, 1.0, -1.0)
    t1h, t1l = np_halves(t1)
    t3h, t3l = np_halves(t3)
    return {
        "data_first": np.concatenate([t1h, t1l], axis=1),
        "kernel_first": np.concatenate([t1h, t1h, t1l], axis=1),
        "last": np.concatenate([t3h, t3h, t3l], axis=1),
        "twist": np.stack([np.cos(twist), np.sin(twist)]).astype(np.float32),
        "ahead": np.stack(np_halves(ahead)),
        "both": np.stack(np_halves(np.concatenate([ahead, mirror], axis=0))),
        "back": np.stack(np_halves(back)),
    }


def short(x, before, after, taps):
    rows = lax.broadcasted_iota(jnp.int32, x.shape, 0)
    size = x.shape[0]
    up = jnp.where(rows == 0, before, pltpu.roll(x, 1, 0))
    down = jnp.where(rows == size - 1, after, pltpu.roll(x, size - 1, 0))
    return taps[0:1] * up + taps[1:2] * x + taps[2:3] * down


def product_kernel(mult, value, before, after, taps_mult, taps_value, out):
    b, a = before[...].astype(F32), after[...].astype(F32)
    m = short(mult[...].astype(F32), b[1:2], a[1:2], taps_mult[...])
    v = short(value[...].astype(F32), b[2:3], a[2:3], taps_value[...])
    out[...] = (v * m).T.astype(BF16)


def gate_kernel(gate, mult, value, before, after, taps_gate, taps_mult, taps_value, skip, gate_out, skip_out):
    b, a = before[...].astype(F32), after[...].astype(F32)
    g = short(gate[...].astype(F32), b[0:1], a[0:1], taps_gate[...])
    m = short(mult[...].astype(F32), b[1:2], a[1:2], taps_mult[...])
    v = short(value[...].astype(F32), b[2:3], a[2:3], taps_value[...])
    gate_out[...] = g.T
    skip_out[...] = (skip[...] * (v * m)).T


def filter_kernel(
    first, second, sides, decay, kernel_first, twist, both, out, stage, left_high, left_low, *, seq_len, width, chunk
):
    hidden = second.shape[0]
    bands = (first.shape[0] - 1) // 2
    group = decay.shape[0] // 2
    blocks = seq_len // width
    padded = 2 * bands + 8
    w1 = jnp.concatenate(
        [first[1 : 1 + 2 * bands, :], first[0:1, :], jnp.zeros((padded - 2 * bands - 1, hidden), F32)], axis=0
    )
    w1h, w1l = halves(w1)
    w1s = jnp.concatenate(
        [w1h.astype(F32), w1h.astype(F32), w1l.astype(F32), jnp.zeros((128 - 3 * padded, hidden), F32)], axis=0
    ).T.astype(BF16)
    w2h, w2l = halves(second[...].T)
    w2s = jnp.concatenate([w2h, w2h, w2l], axis=1)
    w3h, w3l = halves(sides[...].T)
    w3s = jnp.concatenate([w3h, w3h, w3l], axis=1)
    row = lax.broadcasted_iota(jnp.int32, (2 * bands, chunk), 0)
    band_at = jnp.where(row < bands, row, row - bands).astype(F32)
    band = np.float32(0.0001) + band_at * np.float32((bands - 1 - 0.0001) / (bands - 1))
    band = jnp.where(row < bands, band, -band)
    offset = jnp.where(row < bands, np.float32(0.5 * math.pi), np.float32(0.0))
    head_row = lax.broadcasted_iota(jnp.int32, (8, chunk), 0)
    rates = decay[...]

    def step(i, total):
        at = i * chunk
        position = (lax.broadcasted_iota(jnp.int32, (1, chunk), 1) + at).astype(F32)
        tau = position / np.float32(seq_len - 1)
        omega = position * np.float32(2.0 * math.pi / seq_len)
        trig = sine(omega * band + offset)
        feats = jnp.concatenate([trig, jnp.where(head_row == 0, tau, 0.0)], axis=0)
        fh = feats.astype(BF16).astype(F32)
        fs = jnp.concatenate(
            [fh, feats - fh, fh, jnp.zeros((128 - 3 * padded, chunk), F32)], axis=0
        ).astype(BF16)
        h1h, h1l = halves(sine(dot(w1s, fs)))
        h2h, h2l = halves(sine(dot(w2s, jnp.concatenate([h1h, h1l, h1h], axis=0))))
        values = dot(w3s, jnp.concatenate([h2h, h2l, h2h], axis=0))
        values = values * jnp.exp(-rates * tau)
        side_row = lax.broadcasted_iota(jnp.int32, values.shape, 0)
        values = jnp.where((side_row >= group) & (position < 0.5), 0.0, values)
        for j in range(chunk // width):
            part = values[:, j * width : (j + 1) * width]
            total = total + part * part
            start = pl.multiple_of((i * (chunk // width) + j) * 2 * group, 2 * group)
            stage[pl.ds(start, 2 * group), :] = part
        return total

    total = lax.fori_loop(0, seq_len // chunk, step, jnp.zeros((2 * group, width), F32))
    power = jnp.sum(total, axis=1, keepdims=True)
    scale = lax.rsqrt(power[:group] + power[group:] + np.float32(1e-06))
    cos, sin = twist[0], twist[1]
    cos2, sin2 = jnp.concatenate([cos, cos], axis=1), jnp.concatenate([sin, sin], axis=1)
    for c in range(group):
        x = jnp.concatenate(
            [stage[pl.ds(c, blocks, stride=2 * group), :], stage[pl.ds(group + c, blocks, stride=2 * group), :]], axis=1
        )
        xh, xl = halves(x * scale[c : c + 1, :])
        z = dot(kernel_first[...], jnp.concatenate([xh, xl, xh], axis=0))
        re, im = z[:blocks], z[blocks:]
        re, im = re * cos2 + im * sin2, im * cos2 - re * sin2
        left = jnp.concatenate([re[:, :width], im[:, :width], re[:, width:], im[:, width:]], axis=1)
        high, low = halves(left)
        left_high[c * blocks : (c + 1) * blocks, :] = high
        left_low[c * blocks : (c + 1) * blocks, :] = low
    out[...] = dot(left_high[...], both[0]) + dot(left_low[...], both[0]) + dot(left_high[...], both[1])


def conv_kernel(data, spec, data_first, twist, ahead, back, last, out, stage, left_high, left_low, *, group):
    width = data.shape[1]
    blocks = data.shape[0] // group
    cos, sin = twist[0], twist[1]
    stage[...] = data[...].astype(F32)
    for c in range(group):
        x = stage[pl.ds(c, blocks, stride=group), :].astype(BF16)
        z = dot(data_first[...], jnp.concatenate([x, x], axis=0))
        re, im = z[:blocks], z[blocks:]
        left = jnp.concatenate([re * cos + im * sin, im * cos - re * sin], axis=1)
        high, low = halves(left)
        left_high[c * blocks : (c + 1) * blocks, :] = high
        left_low[c * blocks : (c + 1) * blocks, :] = low
    s = dot(left_high[...], ahead[0]) + dot(left_low[...], ahead[0]) + dot(left_high[...], ahead[1])
    sr, si = s[:, :width], s[:, width:]
    kr, ki = spec[:, :width], spec[:, width:]
    high, low = halves(jnp.concatenate([sr * kr - si * ki, sr * ki + si * kr], axis=1))
    v = dot(high, back[0]) + dot(low, back[0]) + dot(high, back[1])
    for c in range(group):
        vr = v[c * blocks : (c + 1) * blocks, :width]
        vi = v[c * blocks : (c + 1) * blocks, width:]
        high, low = halves(jnp.concatenate([vr * cos - vi * sin, vi * cos + vr * sin], axis=0))
        stage[pl.ds(c, blocks, stride=group), :] = dot(last[...], jnp.concatenate([high, low, high], axis=0))
    out[...] = stage[...].astype(BF16)


def body(
    gate_in,
    mult_in,
    value_in,
    taps_gate,
    taps_mult,
    taps_value,
    filter_first,
    filter_second,
    filter_ahead,
    filter_behind,
    filter_decay,
    skip_gain,
    out_weight,
):
    cols = lax.axis_size(COL)
    col = lax.axis_index(COL)
    width, channels = gate_in.shape[1:]
    seq_len = width * cols
    group = channels // cols
    gate, mult, value = gate_in[0], mult_in[0], value_in[0]
    t = tables(cols, width)

    up = [(i, i + 1) for i in range(cols - 1)]
    down = [(j, i) for i, j in up]
    before = lax.ppermute(jnp.concatenate([gate[-1:], mult[-1:], value[-1:]]), COL, up)
    after = lax.ppermute(jnp.concatenate([gate[:1], mult[:1], value[:1]]), COL, down)
    product = pl.pallas_call(product_kernel, out_shape=jax.ShapeDtypeStruct((channels, width), BF16), name="product")(
        mult, value, before, after, taps_mult, taps_value
    )
    spread = lax.all_to_all(product.reshape(cols, group, width), COL, 0, 0, tiled=True)

    first = col * group
    sides = jnp.concatenate(
        [lax.dynamic_slice_in_dim(w, first, group, 1) for w in (filter_ahead, filter_behind)], axis=1
    )
    rates = lax.dynamic_slice_in_dim(filter_decay, first, group)
    rates = jnp.concatenate([rates, rates])[:, None]
    spec = pl.pallas_call(
        functools.partial(filter_kernel, seq_len=seq_len, width=width, chunk=4 * width),
        out_shape=jax.ShapeDtypeStruct((group * cols, 2 * width), F32),
        scratch_shapes=[
            pltpu.VMEM((2 * group * cols, width), F32),
            pltpu.VMEM((group * cols, 4 * width), BF16),
            pltpu.VMEM((group * cols, 4 * width), BF16),
        ],
        name="filter",
    )(filter_first, filter_second, sides, rates, t["kernel_first"], t["twist"], t["both"])
    gate_part, skip_part = pl.pallas_call(
        gate_kernel,
        out_shape=[jax.ShapeDtypeStruct((channels, width), F32)] * 2,
        name="gate",
    )(gate, mult, value, before, after, taps_gate, taps_mult, taps_value, skip_gain[None])

    convolved = pl.pallas_call(
        functools.partial(conv_kernel, group=group),
        out_shape=jax.ShapeDtypeStruct((channels, width), BF16),
        scratch_shapes=[
            pltpu.VMEM((channels, width), F32),
            pltpu.VMEM((channels, 2 * width), BF16),
            pltpu.VMEM((channels, 2 * width), BF16),
        ],
        name="conv",
    )(spread.reshape(channels, width), spec, t["data_first"], t["twist"], t["ahead"], t["back"], t["last"])
    returned = lax.all_to_all(convolved.reshape(cols, group, width), COL, 0, 0, tiled=True)
    gated = ((returned.reshape(channels, width).astype(F32) + skip_part) * gate_part).astype(BF16)
    mixed = lax.dot_general(gated, out_weight, (((0,), (0,)), ((), ())), preferred_element_type=F32)
    return mixed.astype(BF16)[None]


def solution(mesh):
    tokens = P(("grp", "row"), COL, None)
    in_specs = (tokens,) * 3 + (P(),) * 10
    return jax.shard_map(body, mesh=mesh, in_specs=in_specs, out_specs=tokens, check_vma=False)
```

```python
import functools
import math

import jax
import jax.numpy as jnp
import numpy as np
from jax import lax
from jax.experimental import pallas as pl
from jax.experimental.pallas import tpu as pltpu
from jax.sharding import Mesh
from jax.sharding import PartitionSpec as P

CHIP = "col_chip"
CORE = "col_core"
COL = (CHIP, CORE)
CORES = 2
EDGE = 8
F32 = jnp.float32
BF16 = jnp.bfloat16

TWO_PI_HEAD = np.float32(np.round(2.0 * math.pi * 2**14) / 2**14)
TWO_PI_TAIL = np.float32(2.0 * math.pi - float(TWO_PI_HEAD))


def sine_coefficients():
    nodes = np.cos((np.arange(4000) + 0.5) * math.pi / 8000) * math.pi * 1.0001
    basis = np.stack([nodes ** (2 * j + 1) for j in range(7)], axis=1)
    return [float(v) for v in np.linalg.lstsq(basis, np.sin(nodes), rcond=None)[0]]


SINE = sine_coefficients()


def sine(x):
    turns = jnp.floor(x * np.float32(0.5 / math.pi) + 0.5)
    r = (x - turns * TWO_PI_HEAD) - turns * TWO_PI_TAIL
    z = r * r
    total = np.float32(SINE[6]) * z + np.float32(SINE[5])
    for j in (4, 3, 2, 1, 0):
        total = total * z + np.float32(SINE[j])
    return total * r


def halves(x):
    high = x.astype(BF16)
    return high, (x - high.astype(F32)).astype(BF16)


def np_halves(x):
    high = np.asarray(x, np.float32).astype(BF16)
    return high, (np.asarray(x, np.float32) - high.astype(np.float32)).astype(BF16)


def cost(microseconds, size):
    return pl.CostEstimate(flops=int(microseconds * 4e8), bytes_accessed=size, transcendentals=0)


def limit(mebibytes):
    return pltpu.CompilerParams(vmem_limit_bytes=mebibytes * 2**20)


def dot(a, b):
    return jnp.dot(a, b, preferred_element_type=F32)


def tables(blocks, width):
    span = 2 * blocks * width
    freq = np.arange(blocks) + 0.5
    first = 2.0 * math.pi * np.outer(freq, np.arange(blocks)) / (2 * blocks)
    t1 = np.concatenate([np.cos(first), -np.sin(first)], axis=0)
    t3 = np.concatenate([np.cos(first).T, -np.sin(first).T], axis=1) * (2.0 / span)
    twist = 2.0 * math.pi * np.outer(freq, np.arange(width)) / span
    second = 2.0 * math.pi * (np.outer(np.arange(width), np.arange(width)) % width) / width
    c, s = np.cos(second), np.sin(second)
    ahead = np.block([[c, -s], [s, c]])
    back = np.block([[c, s], [-s, c]])
    mirror = ahead * np.where(np.arange(2 * width) < width, 1.0, -1.0)
    t1h, t1l = np_halves(t1)
    t3h, t3l = np_halves(t3)
    return {
        "data_first": np.concatenate([t1h, t1l], axis=1),
        "kernel_first": np.concatenate([t1h, t1h, t1l], axis=1),
        "last": np.concatenate([t3h, t3h, t3l], axis=1),
        "twist": np.stack([np.cos(twist), np.sin(twist)]).astype(np.float32),
        "ahead": np.stack(np_halves(ahead)),
        "both": np.stack(np_halves(np.concatenate([ahead, mirror], axis=0))),
        "back": np.stack(np_halves(back)),
    }


def short(x, before, after, taps):
    rows = lax.broadcasted_iota(jnp.int32, x.shape, 0)
    size = x.shape[0]
    up = jnp.where(rows == 0, before, pltpu.roll(x, 1, 0))
    down = jnp.where(rows == size - 1, after, pltpu.roll(x, size - 1, 0))
    return taps[0:1] * up + taps[1:2] * x + taps[2:3] * down


def product_kernel(mult, value, taps_mult, taps_value, out):
    m, v = mult[...].astype(F32), value[...].astype(F32)
    zero = jnp.zeros((1, m.shape[1]), F32)
    product = short(v, zero, zero, taps_value[...]) * short(m, zero, zero, taps_mult[...])
    product = product.T.astype(BF16)
    edges = jnp.concatenate([v[:2], m[:2], v[-2:], m[-2:]], axis=0).astype(BF16)
    chips, rows, width = out.shape
    part = (rows - EDGE) // 2
    for k in range(chips):
        at = 2 * part * k
        lane = at // width * width
        out[k, :part, :] = product[at : at + part]
        out[k, part : part + EDGE, :] = edges[:, lane : lane + width]
        out[k, part + EDGE :, :] = product[at + part : at + 2 * part]


def gate_kernel(
    gate, mult, value, before, after, taps_gate, taps_mult, taps_value, skip, gate_out, skip_out
):
    b, a = before[...].astype(F32), after[...].astype(F32)
    g = short(gate[...].astype(F32), b[0:1], a[0:1], taps_gate[...])
    m = short(mult[...].astype(F32), b[1:2], a[1:2], taps_mult[...])
    v = short(value[...].astype(F32), b[2:3], a[2:3], taps_value[...])
    gate_out[...] = g
    skip_out[...] = skip[...] * (v * m)


def mix_kernel(planes, other, gate_part, skip_part, weight, out, stage):
    core = lax.axis_index(CORE)
    chips, rows, _ = planes.shape
    group = rows // CORES
    for k in range(chips):
        near = pl.multiple_of(rows * k + core * group, group)
        far = pl.multiple_of(rows * k + (1 - core) * group, group)
        stage[pl.ds(near, group), :] = planes[k, pl.ds(pl.multiple_of(core * group, group), group), :].astype(F32)
        stage[pl.ds(far, group), :] = other[k].astype(F32)
    gated = ((stage[...].T + skip_part[...]) * gate_part[...]).astype(BF16)
    out[...] = dot(gated, weight[...]).astype(BF16)


def filter_kernel(
    *refs, seq_len, width, chunk, group
):
    sources, out, copies, (own, stage, left_high, left_low, sems) = refs[:8], refs[8], refs[9:17], refs[17:]
    moves = [pltpu.make_async_copy(a, b, sems.at[n]) for n, (a, b) in enumerate(zip(sources, copies))]
    for move in moves:
        move.start()
    for move in moves:
        move.wait()
    first, second, ahead, behind, decay, kernel_first, twist, both = copies
    hidden = second.shape[0]
    bands = (first.shape[0] - 1) // 2
    channel = (lax.axis_index(CHIP) * CORES + lax.axis_index(CORE)) * group
    lane = pl.multiple_of(channel // width * width, width)
    row_at = pl.multiple_of(channel % width, group)
    own[0] = ahead[:, pl.ds(lane, width)].T
    own[1] = behind[:, pl.ds(lane, width)].T
    own[2] = jnp.broadcast_to(decay[:, pl.ds(lane, width)], (width, width)).T
    sides = jnp.concatenate([own[0, pl.ds(row_at, group), :], own[1, pl.ds(row_at, group), :]], axis=0)
    rates = own[2, pl.ds(row_at, group), :][:, 0:1]
    rates = jnp.concatenate([rates, rates], axis=0)
    blocks = seq_len // width
    padded = 2 * bands + 8
    w1 = jnp.concatenate(
        [first[1 : 1 + 2 * bands, :], first[0:1, :], jnp.zeros((padded - 2 * bands - 1, hidden), F32)], axis=0
    )
    w1h, w1l = halves(w1)
    w1s = jnp.concatenate(
        [w1h.astype(F32), w1h.astype(F32), w1l.astype(F32), jnp.zeros((128 - 3 * padded, hidden), F32)], axis=0
    ).T.astype(BF16)
    w2h, w2l = halves(second[...].T)
    w2s = jnp.concatenate([w2h, w2h, w2l], axis=1)
    w3h, w3l = halves(sides)
    w3s = jnp.concatenate([w3h, w3h, w3l], axis=1)
    row = lax.broadcasted_iota(jnp.int32, (2 * bands, chunk), 0)
    band_at = jnp.where(row < bands, row, row - bands).astype(F32)
    band = np.float32(0.0001) + band_at * np.float32((bands - 1 - 0.0001) / (bands - 1))
    band = jnp.where(row < bands, band, -band)
    offset = jnp.where(row < bands, np.float32(0.5 * math.pi), np.float32(0.0))
    head_row = lax.broadcasted_iota(jnp.int32, (8, chunk), 0)

    def step(i, total):
        at = i * chunk
        position = (lax.broadcasted_iota(jnp.int32, (1, chunk), 1) + at).astype(F32)
        tau = position / np.float32(seq_len - 1)
        omega = position * np.float32(2.0 * math.pi / seq_len)
        trig = sine(omega * band + offset)
        feats = jnp.concatenate([trig, jnp.where(head_row == 0, tau, 0.0)], axis=0)
        fh = feats.astype(BF16).astype(F32)
        fs = jnp.concatenate(
            [fh, feats - fh, fh, jnp.zeros((128 - 3 * padded, chunk), F32)], axis=0
        ).astype(BF16)
        h1h, h1l = halves(sine(dot(w1s, fs)))
        h2h, h2l = halves(sine(dot(w2s, jnp.concatenate([h1h, h1l, h1h], axis=0))))
        values = dot(w3s, jnp.concatenate([h2h, h2l, h2h], axis=0))
        values = values * jnp.exp(-rates * tau)
        side_row = lax.broadcasted_iota(jnp.int32, values.shape, 0)
        values = jnp.where((side_row >= group) & (position < 0.5), 0.0, values)
        for j in range(chunk // width):
            part = values[:, j * width : (j + 1) * width]
            total = total + part * part
            start = pl.multiple_of((i * (chunk // width) + j) * 2 * group, 2 * group)
            stage[pl.ds(start, 2 * group), :] = part
        return total

    total = lax.fori_loop(0, seq_len // chunk, step, jnp.zeros((2 * group, width), F32))
    power = jnp.sum(total, axis=1, keepdims=True)
    scale = lax.rsqrt(power[:group] + power[group:] + np.float32(1e-06))
    cos, sin = twist[0], twist[1]
    cos2, sin2 = jnp.concatenate([cos, cos], axis=1), jnp.concatenate([sin, sin], axis=1)
    for c in range(group):
        x = jnp.concatenate(
            [stage[pl.ds(c, blocks, stride=2 * group), :], stage[pl.ds(group + c, blocks, stride=2 * group), :]], axis=1
        )
        xh, xl = halves(x * scale[c : c + 1, :])
        z = dot(kernel_first[...], jnp.concatenate([xh, xl, xh], axis=0))
        re, im = z[:blocks], z[blocks:]
        re, im = re * cos2 + im * sin2, im * cos2 - re * sin2
        left = jnp.concatenate([re[:, :width], im[:, :width], re[:, width:], im[:, width:]], axis=1)
        high, low = halves(left)
        left_high[c * blocks : (c + 1) * blocks, :] = high
        left_low[c * blocks : (c + 1) * blocks, :] = low
    out[...] = dot(left_high[...], both[0]) + dot(left_low[...], both[0]) + dot(left_high[...], both[1])


def conv_kernel(
    plane, partner, taps_mult, taps_value, spec, data_first, twist, ahead, back, last, out, stage, left_high, left_low,
    *, group
):
    chips, rows, width = partner.shape
    blocks = chips * CORES
    chip, core = lax.axis_index(CHIP), lax.axis_index(CORE)
    pitch = group + 2 * EDGE
    base = pl.multiple_of(EDGE * (1 - core), EDGE)
    own_at = pl.multiple_of(core * group, group)
    for k in range(chips):
        near = pl.multiple_of((CORES * k + core) * pitch + base, EDGE)
        far = pl.multiple_of((CORES * k + 1 - core) * pitch + base, EDGE)
        stage[pl.ds(near, rows), :] = plane[k, pl.ds(own_at, rows), :].astype(F32)
        stage[pl.ds(far, rows), :] = partner[k].astype(F32)

    channel = (chip * CORES + core) * group
    lane = pl.multiple_of(channel // width * width, width)
    tm, tv = taps_mult[:, pl.ds(lane, width)], taps_value[:, pl.ds(lane, width)]
    edge_at = (group + EDGE) * (1 - core)
    v0, v1, m0, m1, v2, v3, m2, m3 = [stage[pl.ds(edge_at + q, blocks, stride=pitch), :] for q in range(EDGE)]
    row = lax.broadcasted_iota(jnp.int32, (blocks, width), 0)
    column = lax.broadcasted_iota(jnp.int32, (blocks, width), 1)

    def head(t, previous, x, following):
        return t[0:1] * jnp.where(row == 0, 0.0, pltpu.roll(previous, 1, 0)) + t[1:2] * x + t[2:3] * following

    def tail(t, previous, x, following):
        after = jnp.where(row == blocks - 1, 0.0, pltpu.roll(following, blocks - 1, 0))
        return t[0:1] * previous + t[1:2] * x + t[2:3] * after

    heads = head(tv, v3, v0, v1) * head(tm, m3, m0, m1)
    tails = tail(tv, v2, v3, v0) * tail(tm, m2, m3, m0)
    shift = width - channel % width
    heads = pltpu.roll(heads, shift, 1)
    tails = pltpu.roll(tails, shift + width - 1, 1)
    odd = column % 2 == 1
    edges = (jnp.where(odd, tails, heads), jnp.where(odd, heads, tails))
    border = (column == 0) | (column == width - 1)

    cos, sin = twist[0], twist[1]
    for c in range(group):
        x = stage[pl.ds(EDGE + c, blocks, stride=pitch), :]
        x = jnp.where(border, pltpu.roll(edges[c % 2], (width - c) % width, 1), x).astype(BF16)
        z = dot(data_first[...], jnp.concatenate([x, x], axis=0))
        re, im = z[:blocks], z[blocks:]
        left = jnp.concatenate([re * cos + im * sin, im * cos - re * sin], axis=1)
        high, low = halves(left)
        left_high[c * blocks : (c + 1) * blocks, :] = high
        left_low[c * blocks : (c + 1) * blocks, :] = low
    s = dot(left_high[...], ahead[0]) + dot(left_low[...], ahead[0]) + dot(left_high[...], ahead[1])
    sr, si = s[:, :width], s[:, width:]
    kr, ki = spec[:, :width], spec[:, width:]
    high, low = halves(jnp.concatenate([sr * kr - si * ki, sr * ki + si * kr], axis=1))
    v = dot(high, back[0]) + dot(low, back[0]) + dot(high, back[1])
    for c in range(group):
        vr = v[c * blocks : (c + 1) * blocks, :width]
        vi = v[c * blocks : (c + 1) * blocks, width:]
        high, low = halves(jnp.concatenate([vr * cos - vi * sin, vi * cos + vr * sin], axis=0))
        stage[pl.ds(c, blocks, stride=group), :] = dot(last[...], jnp.concatenate([high, low, high], axis=0))
    out[...] = stage[: blocks * group, :].astype(BF16)


def body(
    gate_in,
    mult_in,
    value_in,
    taps_gate,
    taps_mult,
    taps_value,
    filter_first,
    filter_second,
    filter_ahead,
    filter_behind,
    filter_decay,
    skip_gain,
    out_weight,
):
    chips, core = lax.axis_size(CHIP), lax.axis_index(CORE)
    cols = chips * CORES
    width, channels = gate_in.shape[1:]
    seq_len = width * cols
    group = channels // cols
    gate, mult, value = gate_in[0], mult_in[0], value_in[0]
    t = tables(cols, width)
    swap = [(i, i + 1 - 2 * (i % CORES)) for i in range(cols)]
    up = [(i, i + 1) for i in range(cols - 1)]
    down = [(j, i) for i, j in up]

    rows = CORES * group + EDGE
    product = pl.pallas_call(
        product_kernel,
        out_shape=jax.ShapeDtypeStruct((chips, rows, width), BF16),
        compiler_params=pltpu.CompilerParams(vmem_limit_bytes=67_000_000),
        name="product",
    )(mult, value, taps_mult, taps_value)
    plane = lax.all_to_all(product, CHIP, 0, 0, tiled=True)
    filter_args = (
        filter_first, filter_second, filter_ahead, filter_behind, filter_decay[None], t["kernel_first"], t["twist"], t["both"]
    )
    spec = pl.pallas_call(
        functools.partial(filter_kernel, seq_len=seq_len, width=width, chunk=4 * width, group=group),
        in_specs=[pl.BlockSpec(memory_space=pltpu.HBM)] * len(filter_args),
        out_shape=jax.ShapeDtypeStruct((group * cols, 2 * width), F32),
        scratch_shapes=[pltpu.VMEM(x.shape, x.dtype) for x in filter_args]
        + [
            pltpu.VMEM((3, width, width), F32),
            pltpu.VMEM((2 * group * cols, width), F32),
            pltpu.VMEM((group * cols, 4 * width), BF16),
            pltpu.VMEM((group * cols, 4 * width), BF16),
            pltpu.SemaphoreType.DMA((len(filter_args),)),
        ],
        compiler_params=limit(16),
        cost_estimate=cost(10, 2**22),
        name="filter",
    )(*filter_args)
    plane, spec = lax.optimization_barrier((plane, spec))
    partner = lax.ppermute(lax.dynamic_slice_in_dim(plane, (1 - core) * group, group + EDGE, 1), COL, swap)

    convolved = pl.pallas_call(
        functools.partial(conv_kernel, group=group),
        out_shape=jax.ShapeDtypeStruct((channels, width), BF16),
        scratch_shapes=[
            pltpu.VMEM((cols * (group + 2 * EDGE), width), F32),
            pltpu.VMEM((channels, 2 * width), BF16),
            pltpu.VMEM((channels, 2 * width), BF16),
        ],
        compiler_params=limit(16),
        cost_estimate=cost(3, 2**21),
        name="conv",
    )(plane, partner, taps_mult, taps_value, spec, t["data_first"], t["twist"], t["ahead"], t["back"], t["last"])

    convolved, gate, mult, value = lax.optimization_barrier((convolved, gate, mult, value))
    planes = lax.all_to_all(convolved.reshape(chips, CORES * group, width), CHIP, 0, 0, tiled=True)
    before = lax.ppermute(jnp.concatenate([gate[-1:], mult[-1:], value[-1:]]), COL, up)
    after = lax.ppermute(jnp.concatenate([gate[:1], mult[:1], value[:1]]), COL, down)
    gate_part, skip_part = pl.pallas_call(
        gate_kernel,
        out_shape=[jax.ShapeDtypeStruct((width, channels), F32)] * 2,
        compiler_params=limit(12),
        cost_estimate=cost(20, 2**21),
        name="gate",
    )(gate, mult, value, before, after, taps_gate, taps_mult, taps_value, skip_gain[None])
    planes, gate_part, skip_part = lax.optimization_barrier((planes, gate_part, skip_part))
    theirs = lax.dynamic_slice_in_dim(planes, (1 - core) * group, group, 1)
    other = lax.ppermute(theirs, COL, swap)
    mixed = pl.pallas_call(
        mix_kernel,
        out_shape=jax.ShapeDtypeStruct((width, out_weight.shape[1]), BF16),
        scratch_shapes=[pltpu.VMEM((channels, width), F32)],
        compiler_params=limit(12),
        cost_estimate=cost(2, 2**22),
        name="mix",
    )(planes, other, gate_part, skip_part, out_weight)
    return mixed[None]


def solution(mesh):
    shape = mesh.shape
    split = Mesh(
        mesh.devices.reshape(shape["grp"], shape["row"], shape["col"] // CORES, CORES), ("grp", "row", CHIP, CORE)
    )
    tokens = P(("grp", "row"), COL, None)
    in_specs = (tokens,) * 3 + (P(),) * 10
    return jax.shard_map(body, mesh=split, in_specs=in_specs, out_specs=tokens, check_vma=False)
```

```python
import functools
import math

import jax
import jax.numpy as jnp
import numpy as np
from jax import lax
from jax.experimental import pallas as pl
from jax.experimental.pallas import tpu as pltpu
from jax.sharding import Mesh
from jax.sharding import PartitionSpec as P

CHIP = "col_chip"
CORE = "col_core"
COL = (CHIP, CORE)
CORES = 2
EDGE = 8
ALL_VMEM = 67_000_000
F32 = jnp.float32
BF16 = jnp.bfloat16

TWO_PI_HEAD = np.float32(np.round(2.0 * math.pi * 2**14) / 2**14)
TWO_PI_TAIL = np.float32(2.0 * math.pi - float(TWO_PI_HEAD))


def sine_coefficients():
    nodes = np.cos((np.arange(4000) + 0.5) * math.pi / 8000) * math.pi * 1.0001
    basis = np.stack([nodes ** (2 * j + 1) for j in range(7)], axis=1)
    return [float(v) for v in np.linalg.lstsq(basis, np.sin(nodes), rcond=None)[0]]


SINE = sine_coefficients()


def sine(x):
    turns = jnp.floor(x * np.float32(0.5 / math.pi) + 0.5)
    r = (x - turns * TWO_PI_HEAD) - turns * TWO_PI_TAIL
    z = r * r
    total = np.float32(SINE[6]) * z + np.float32(SINE[5])
    for j in (4, 3, 2, 1, 0):
        total = total * z + np.float32(SINE[j])
    return total * r


def halves(x):
    high = x.astype(BF16)
    return high, (x - high.astype(F32)).astype(BF16)


def np_halves(x):
    high = np.asarray(x, np.float32).astype(BF16)
    return high, (np.asarray(x, np.float32) - high.astype(np.float32)).astype(BF16)


def cost(microseconds, size):
    return pl.CostEstimate(flops=int(microseconds * 4e8), bytes_accessed=size, transcendentals=0)


def limit(mebibytes):
    return pltpu.CompilerParams(vmem_limit_bytes=mebibytes * 2**20)


def dot(a, b):
    return jnp.dot(a, b, preferred_element_type=F32)


def tables(blocks, width):
    span = 2 * blocks * width
    freq = np.arange(blocks) + 0.5
    first = 2.0 * math.pi * np.outer(freq, np.arange(blocks)) / (2 * blocks)
    t1 = np.concatenate([np.cos(first), -np.sin(first)], axis=0)
    t3 = np.concatenate([np.cos(first).T, -np.sin(first).T], axis=1) * (2.0 / span)
    twist = 2.0 * math.pi * np.outer(freq, np.arange(width)) / span
    second = 2.0 * math.pi * (np.outer(np.arange(width), np.arange(width)) % width) / width
    c, s = np.cos(second), np.sin(second)
    ahead = np.block([[c, -s], [s, c]])
    back = np.block([[c, s], [-s, c]])
    mirror = ahead * np.where(np.arange(2 * width) < width, 1.0, -1.0)
    t1h, t1l = np_halves(t1)
    t3h, t3l = np_halves(t3)
    return {
        "data_first": np.concatenate([t1h, t1l], axis=1),
        "kernel_first": np.concatenate([t1h, t1h, t1l], axis=1),
        "last": np.concatenate([t3h, t3h, t3l], axis=1),
        "twist": np.stack([np.cos(twist), np.sin(twist)]).astype(np.float32),
        "ahead": np.stack(np_halves(ahead)),
        "both": np.stack(np_halves(np.concatenate([ahead, mirror], axis=0))),
        "back": np.stack(np_halves(back)),
    }


def short(x, before, after, taps):
    rows = lax.broadcasted_iota(jnp.int32, x.shape, 0)
    size = x.shape[0]
    up = jnp.where(rows == 0, before, pltpu.roll(x, 1, 0))
    down = jnp.where(rows == size - 1, after, pltpu.roll(x, size - 1, 0))
    return taps[0:1] * up + taps[1:2] * x + taps[2:3] * down


def product_kernel(mult, value, gate_head, gate_tail, taps_mult, taps_value, out):
    m, v = mult[...].astype(F32), value[...].astype(F32)
    product = (short(v, 0.0, 0.0, taps_value[...]) * short(m, 0.0, 0.0, taps_mult[...])).T.astype(BF16)
    zero = jnp.zeros((EDGE - 6, m.shape[1]), F32)
    heads = jnp.concatenate([v[:2], m[:2], gate_head[...].astype(F32)[:2], zero], axis=0)
    tails = jnp.concatenate([v[-2:], m[-2:], gate_tail[...].astype(F32)[-2:], zero], axis=0)
    chips, rows, width = out.shape
    part = (rows - EDGE) // CORES
    half = CORES * part
    low = lax.broadcasted_iota(jnp.int32, (EDGE, width), 1) < half
    for k in range(chips):
        at = half * k
        lane = at // width * width
        head, tail = heads[:, lane : lane + width], tails[:, lane : lane + width]
        if at == lane:
            tail = pltpu.roll(tail, half, 1)
        else:
            head = pltpu.roll(head, half, 1)
        out[k, :part, :] = product[at : at + part]
        out[k, part : part + EDGE, :] = jnp.where(low, head, tail).astype(BF16)
        out[k, part + EDGE :, :] = product[at + part : at + half]


def gains_kernel(taps_mult, taps_value, taps_gate, skip, out):
    width = out.shape[1]
    group = width // 4
    channel = (lax.axis_index(CHIP) * CORES + lax.axis_index(CORE)) * group
    lane = pl.multiple_of(channel // width * width, width)
    gains = [r[:, pl.ds(lane, width)] for r in (taps_mult, taps_value, taps_gate, skip)]
    gains = jnp.concatenate(gains + [jnp.zeros((out.shape[0] - 10, width), F32)], axis=0)
    out[...] = pltpu.roll(gains, (width - channel % width) % width, 1)


def mix_kernel(planes, other, gate, mult, value, taps_gate, taps_mult, taps_value, skip, weight, out, stage):
    core = lax.axis_index(CORE)
    chips, rows, _ = planes.shape
    group = rows // CORES
    for k in range(chips):
        near = pl.multiple_of(rows * k + core * group, group)
        far = pl.multiple_of(rows * k + (1 - core) * group, group)
        stage[pl.ds(near, group), :] = planes[k, pl.ds(pl.multiple_of(core * group, group), group), :].astype(F32)
        stage[pl.ds(far, group), :] = other[k].astype(F32)
    q = stage[...].T
    row = lax.broadcasted_iota(jnp.int32, q.shape, 0)
    border = (row == 0) | (row == q.shape[0] - 1)
    product = short(value[...].astype(F32), 0.0, 0.0, taps_value[...]) * short(mult[...].astype(F32), 0.0, 0.0, taps_mult[...])
    g = short(gate[...].astype(F32), 0.0, 0.0, taps_gate[...])
    gated = jnp.where(border, q, (q + skip[...] * product) * g).astype(BF16)
    out[...] = dot(gated, weight[...]).astype(BF16)


def filter_kernel(
    *refs, seq_len, width, chunk, group
):
    sources, out, copies, (own, stage, left_high, left_low, sems) = refs[:8], refs[8], refs[9:17], refs[17:]
    moves = [pltpu.make_async_copy(a, b, sems.at[n]) for n, (a, b) in enumerate(zip(sources, copies))]
    for move in moves:
        move.start()
    for move in moves:
        move.wait()
    first, second, ahead, behind, decay, kernel_first, twist, both = copies
    hidden = second.shape[0]
    bands = (first.shape[0] - 1) // 2
    channel = (lax.axis_index(CHIP) * CORES + lax.axis_index(CORE)) * group
    lane = pl.multiple_of(channel // width * width, width)
    row_at = pl.multiple_of(channel % width, group)
    own[0] = ahead[:, pl.ds(lane, width)].T
    own[1] = behind[:, pl.ds(lane, width)].T
    own[2] = jnp.broadcast_to(decay[:, pl.ds(lane, width)], (width, width)).T
    sides = jnp.concatenate([own[0, pl.ds(row_at, group), :], own[1, pl.ds(row_at, group), :]], axis=0)
    rates = own[2, pl.ds(row_at, group), :][:, 0:1]
    rates = jnp.concatenate([rates, rates], axis=0)
    blocks = seq_len // width
    padded = 2 * bands + 8
    w1 = jnp.concatenate(
        [first[1 : 1 + 2 * bands, :], first[0:1, :], jnp.zeros((padded - 2 * bands - 1, hidden), F32)], axis=0
    )
    w1h, w1l = halves(w1)
    w1s = jnp.concatenate(
        [w1h.astype(F32), w1h.astype(F32), w1l.astype(F32), jnp.zeros((128 - 3 * padded, hidden), F32)], axis=0
    ).T.astype(BF16)
    w2h, w2l = halves(second[...].T)
    w2s = jnp.concatenate([w2h, w2h, w2l], axis=1)
    w3h, w3l = halves(sides)
    w3s = jnp.concatenate([w3h, w3h, w3l], axis=1)
    row = lax.broadcasted_iota(jnp.int32, (2 * bands, chunk), 0)
    band_at = jnp.where(row < bands, row, row - bands).astype(F32)
    band = np.float32(0.0001) + band_at * np.float32((bands - 1 - 0.0001) / (bands - 1))
    band = jnp.where(row < bands, band, -band)
    offset = jnp.where(row < bands, np.float32(0.5 * math.pi), np.float32(0.0))
    head_row = lax.broadcasted_iota(jnp.int32, (8, chunk), 0)

    def step(i, total):
        at = i * chunk
        position = (lax.broadcasted_iota(jnp.int32, (1, chunk), 1) + at).astype(F32)
        tau = position / np.float32(seq_len - 1)
        omega = position * np.float32(2.0 * math.pi / seq_len)
        trig = sine(omega * band + offset)
        feats = jnp.concatenate([trig, jnp.where(head_row == 0, tau, 0.0)], axis=0)
        fh = feats.astype(BF16).astype(F32)
        fs = jnp.concatenate(
            [fh, feats - fh, fh, jnp.zeros((128 - 3 * padded, chunk), F32)], axis=0
        ).astype(BF16)
        h1h, h1l = halves(sine(dot(w1s, fs)))
        h2h, h2l = halves(sine(dot(w2s, jnp.concatenate([h1h, h1l, h1h], axis=0))))
        values = dot(w3s, jnp.concatenate([h2h, h2l, h2h], axis=0))
        values = values * jnp.exp(-rates * tau)
        side_row = lax.broadcasted_iota(jnp.int32, values.shape, 0)
        values = jnp.where((side_row >= group) & (position < 0.5), 0.0, values)
        for j in range(chunk // width):
            part = values[:, j * width : (j + 1) * width]
            total = total + part * part
            start = pl.multiple_of((i * (chunk // width) + j) * 2 * group, 2 * group)
            stage[pl.ds(start, 2 * group), :] = part
        return total

    total = lax.fori_loop(0, seq_len // chunk, step, jnp.zeros((2 * group, width), F32))
    power = jnp.sum(total, axis=1, keepdims=True)
    scale = lax.rsqrt(power[:group] + power[group:] + np.float32(1e-06))
    cos, sin = twist[0], twist[1]
    cos2, sin2 = jnp.concatenate([cos, cos], axis=1), jnp.concatenate([sin, sin], axis=1)
    for c in range(group):
        x = jnp.concatenate(
            [stage[pl.ds(c, blocks, stride=2 * group), :], stage[pl.ds(group + c, blocks, stride=2 * group), :]], axis=1
        )
        xh, xl = halves(x * scale[c : c + 1, :])
        z = dot(kernel_first[...], jnp.concatenate([xh, xl, xh], axis=0))
        re, im = z[:blocks], z[blocks:]
        re, im = re * cos2 + im * sin2, im * cos2 - re * sin2
        left = jnp.concatenate([re[:, :width], im[:, :width], re[:, width:], im[:, width:]], axis=1)
        high, low = halves(left)
        left_high[c * blocks : (c + 1) * blocks, :] = high
        left_low[c * blocks : (c + 1) * blocks, :] = low
    out[...] = dot(left_high[...], both[0]) + dot(left_low[...], both[0]) + dot(left_high[...], both[1])


def conv_kernel(
    plane, partner, gains, spec, data_first, twist, ahead, back, last,
    out, stage, left_high, left_low, *, group
):
    chips, rows, width = partner.shape
    blocks = chips * CORES
    core = lax.axis_index(CORE)
    pitch = group + 2 * EDGE
    base = pl.multiple_of(EDGE * (1 - core), EDGE)
    own_at = pl.multiple_of(core * group, group)
    for k in range(chips):
        near = pl.multiple_of((CORES * k + core) * pitch + base, EDGE)
        far = pl.multiple_of((CORES * k + 1 - core) * pitch + base, EDGE)
        stage[pl.ds(near, rows), :] = plane[k, pl.ds(own_at, rows), :].astype(F32)
        stage[pl.ds(far, rows), :] = partner[k].astype(F32)

    tm, tv, tg, gain = gains[0:3], gains[3:6], gains[6:9], gains[9:10]
    edge_at = (group + EDGE) * (1 - core)
    first = [
        pltpu.roll(stage[pl.ds(edge_at + q, blocks, stride=pitch), :], (width - core * group) % width, 1) for q in range(6)
    ]
    v0, v1, m0, m1, g0, g1 = first
    v2, v3, m2, m3, g2, g3 = [pltpu.roll(x, width - CORES * group, 1) for x in first]
    row = lax.broadcasted_iota(jnp.int32, (blocks, width), 0)
    column = lax.broadcasted_iota(jnp.int32, (blocks, width), 1)

    def head(t, previous, x, following):
        return t[0:1] * jnp.where(row == 0, 0.0, pltpu.roll(previous, 1, 0)) + t[1:2] * x + t[2:3] * following

    def tail(t, previous, x, following):
        after = jnp.where(row == blocks - 1, 0.0, pltpu.roll(following, blocks - 1, 0))
        return t[0:1] * previous + t[1:2] * x + t[2:3] * after

    odd = column % 2 == 1

    def pair(heads, tails):
        tails = pltpu.roll(tails, width - 1, 1)
        return jnp.where(odd, tails, heads), jnp.where(odd, heads, tails)

    def at_ends(pairs, c):
        return pltpu.roll(pairs[c % 2], (width - c) % width, 1)

    heads = head(tv, v3, v0, v1) * head(tm, m3, m0, m1)
    tails = tail(tv, v2, v3, v0) * tail(tm, m2, m3, m0)
    edges = pair(heads, tails)
    skips = pair(gain * heads, gain * tails)
    gates = pair(head(tg, g3, g0, g1), tail(tg, g2, g3, g0))
    border = (column == 0) | (column == width - 1)

    cos, sin = twist[0], twist[1]
    for c in range(group):
        x = stage[pl.ds(EDGE + c, blocks, stride=pitch), :]
        x = jnp.where(border, at_ends(edges, c), x).astype(BF16)
        z = dot(data_first[...], jnp.concatenate([x, x], axis=0))
        re, im = z[:blocks], z[blocks:]
        left = jnp.concatenate([re * cos + im * sin, im * cos - re * sin], axis=1)
        high, low = halves(left)
        left_high[c * blocks : (c + 1) * blocks, :] = high
        left_low[c * blocks : (c + 1) * blocks, :] = low
    s = dot(left_high[...], ahead[0]) + dot(left_low[...], ahead[0]) + dot(left_high[...], ahead[1])
    sr, si = s[:, :width], s[:, width:]
    kr, ki = spec[:, :width], spec[:, width:]
    high, low = halves(jnp.concatenate([sr * kr - si * ki, sr * ki + si * kr], axis=1))
    v = dot(high, back[0]) + dot(low, back[0]) + dot(high, back[1])
    for c in range(group):
        vr = v[c * blocks : (c + 1) * blocks, :width]
        vi = v[c * blocks : (c + 1) * blocks, width:]
        high, low = halves(jnp.concatenate([vr * cos - vi * sin, vi * cos + vr * sin], axis=0))
        y = dot(last[...], jnp.concatenate([high, low, high], axis=0))
        y = jnp.where(border, (y + at_ends(skips, c)) * at_ends(gates, c), y)
        stage[pl.ds(c, blocks, stride=group), :] = y
    out[...] = stage[: blocks * group, :].astype(BF16)


def body(
    gate_in,
    mult_in,
    value_in,
    taps_gate,
    taps_mult,
    taps_value,
    filter_first,
    filter_second,
    filter_ahead,
    filter_behind,
    filter_decay,
    skip_gain,
    out_weight,
):
    chips, core = lax.axis_size(CHIP), lax.axis_index(CORE)
    cols = chips * CORES
    width, channels = gate_in.shape[1:]
    seq_len = width * cols
    group = channels // cols
    gate, mult, value = gate_in[0], mult_in[0], value_in[0]
    t = tables(cols, width)
    swap = [(i, i + 1 - 2 * (i % CORES)) for i in range(cols)]

    rows = CORES * group + EDGE
    theirs_at = ((1 - core) * group).astype(jnp.uint32)
    whole = lambda x: pl.BlockSpec(x.shape, lambda i: (0, 0))
    strip = 16
    product = pl.pallas_call(
        product_kernel,
        grid=(1,),
        in_specs=[
            whole(mult),
            whole(value),
            pl.BlockSpec((strip, channels), lambda i: (0, 0)),
            pl.BlockSpec((strip, channels), lambda i: (width // strip - 1, 0)),
            whole(taps_mult),
            whole(taps_value),
        ],
        out_specs=pl.BlockSpec((chips, rows, width), lambda i: (0, 0, 0)),
        out_shape=jax.ShapeDtypeStruct((chips, rows, width), BF16),
        compiler_params=pltpu.CompilerParams(vmem_limit_bytes=ALL_VMEM),
        name="product",
    )(mult, value, gate, gate, taps_mult, taps_value)
    plane = lax.all_to_all(product, CHIP, 0, 0, tiled=True)
    filter_args = (
        filter_first, filter_second, filter_ahead, filter_behind, filter_decay[None], t["kernel_first"], t["twist"], t["both"]
    )
    spec = pl.pallas_call(
        functools.partial(filter_kernel, seq_len=seq_len, width=width, chunk=4 * width, group=group),
        in_specs=[pl.BlockSpec(memory_space=pltpu.HBM)] * len(filter_args),
        out_shape=jax.ShapeDtypeStruct((group * cols, 2 * width), F32),
        scratch_shapes=[pltpu.VMEM(x.shape, x.dtype) for x in filter_args]
        + [
            pltpu.VMEM((3, width, width), F32),
            pltpu.VMEM((2 * group * cols, width), F32),
            pltpu.VMEM((group * cols, 4 * width), BF16),
            pltpu.VMEM((group * cols, 4 * width), BF16),
            pltpu.SemaphoreType.DMA((len(filter_args),)),
        ],
        compiler_params=pltpu.CompilerParams(vmem_limit_bytes=ALL_VMEM),
        cost_estimate=cost(10, 2**22),
        name="filter",
    )(*filter_args)
    spec, taps_near, gain_near = lax.optimization_barrier((spec, (taps_mult, taps_value, taps_gate), skip_gain[None]))
    gains = pl.pallas_call(
        gains_kernel,
        out_shape=jax.ShapeDtypeStruct((16, width), F32),
        compiler_params=limit(1),
        cost_estimate=cost(20, 2**21),
        name="gains",
    )(*taps_near, gain_near)
    plane, spec, gains = lax.optimization_barrier((plane, spec, gains))
    partner = lax.ppermute(lax.dynamic_slice_in_dim(plane, theirs_at, group + EDGE, 1), COL, swap)

    convolved = pl.pallas_call(
        functools.partial(conv_kernel, group=group),
        out_shape=jax.ShapeDtypeStruct((channels, width), BF16),
        scratch_shapes=[
            pltpu.VMEM((cols * (group + 2 * EDGE), width), F32),
            pltpu.VMEM((channels, 2 * width), BF16),
            pltpu.VMEM((channels, 2 * width), BF16),
        ],
        compiler_params=limit(16),
        cost_estimate=cost(3, 2**21),
        name="conv",
    )(plane, partner, gains, spec, t["data_first"], t["twist"], t["ahead"], t["back"], t["last"])

    planes = lax.all_to_all(convolved.reshape(chips, CORES * group, width), CHIP, 0, 0, tiled=True)
    theirs = lax.dynamic_slice_in_dim(planes, theirs_at, group, 1)
    other = lax.ppermute(theirs, COL, swap)
    mixed = pl.pallas_call(
        mix_kernel,
        out_shape=jax.ShapeDtypeStruct((width, out_weight.shape[1]), BF16),
        scratch_shapes=[pltpu.VMEM((channels, width), F32)],
        compiler_params=limit(12),
        cost_estimate=cost(2, 2**22),
        name="mix",
    )(planes, other, gate, mult, value, taps_gate, taps_mult, taps_value, skip_gain[None], out_weight)
    return mixed[None]


def solution(mesh):
    shape = mesh.shape
    split = Mesh(
        mesh.devices.reshape(shape["grp"], shape["row"], shape["col"] // CORES, CORES), ("grp", "row", CHIP, CORE)
    )
    tokens = P(("grp", "row"), COL, None)
    in_specs = (tokens,) * 3 + (P(),) * 10
    return jax.shard_map(body, mesh=split, in_specs=in_specs, out_specs=tokens, check_vma=False)
```

```python
import functools
import math

import jax
import jax.numpy as jnp
import numpy as np
from jax import lax
from jax.experimental import pallas as pl
from jax.experimental.pallas import tpu as pltpu
from jax.sharding import Mesh
from jax.sharding import PartitionSpec as P

CHIP = "col_chip"
CORE = "col_core"
COL = (CHIP, CORE)
CORES = 2
EDGE = 8
ALL_VMEM = 67_000_000
F32 = jnp.float32
BF16 = jnp.bfloat16

def sine_coefficients(terms):
    nodes = np.cos((np.arange(4000) + 0.5) * math.pi / 8000) * 0.25
    basis = np.stack([nodes ** (2 * j + 1) for j in range(terms)], axis=1)
    return [np.float32(v) for v in np.linalg.lstsq(basis, np.sin(2.0 * math.pi * nodes), rcond=None)[0]]


SINE = sine_coefficients(4)
QUARTER = np.float32(0.25)


def cosine_of_turns(u):
    w = QUARTER - jnp.abs(u - jnp.round(u))
    z = w * w
    total = SINE[-1] * z + SINE[-2]
    for c in SINE[-3::-1]:
        total = total * z + c
    return total * w


def sine_of_turns(t):
    return cosine_of_turns(t - QUARTER)


def halves(x):
    high = x.astype(BF16)
    return high, (x - high.astype(F32)).astype(BF16)


def np_halves(x):
    high = np.asarray(x, np.float32).astype(BF16)
    return high, (np.asarray(x, np.float32) - high.astype(np.float32)).astype(BF16)


def cost(microseconds, size):
    return pl.CostEstimate(flops=int(microseconds * 4e8), bytes_accessed=size, transcendentals=0)


def limit(mebibytes):
    return pltpu.CompilerParams(vmem_limit_bytes=mebibytes * 2**20)


def dot(a, b):
    return jnp.dot(a, b, preferred_element_type=F32)


def tables(blocks, width):
    span = 2 * blocks * width
    freq = np.arange(blocks) + 0.5
    first = 2.0 * math.pi * np.outer(freq, np.arange(blocks)) / (2 * blocks)
    t1 = np.concatenate([np.cos(first), -np.sin(first)], axis=0)
    t3 = np.concatenate([np.cos(first).T, -np.sin(first).T], axis=1) * (2.0 / span)
    twist = 2.0 * math.pi * np.outer(freq, np.arange(width)) / span
    second = 2.0 * math.pi * (np.outer(np.arange(width), np.arange(width)) % width) / width
    c, s = np.cos(second), np.sin(second)
    ahead = np.block([[c, -s], [s, c]])
    back = np.block([[c, s], [-s, c]])
    mirror = ahead * np.where(np.arange(2 * width) < width, 1.0, -1.0)
    t1h, t1l = np_halves(t1)
    t3h, t3l = np_halves(t3)
    return {
        "data_first": np.concatenate([t1h, t1l], axis=1),
        "kernel_first": np.concatenate([t1h, t1h, t1l], axis=1),
        "last": np.concatenate([t3h, t3h, t3l], axis=1),
        "twist": np.stack([np.cos(twist), np.sin(twist)]).astype(np.float32),
        "ahead": np.stack(np_halves(ahead)),
        "both": np.stack(np_halves(np.concatenate([ahead, mirror], axis=0))),
        "back": np.stack(np_halves(back)),
    }


def short(x, before, after, taps):
    rows = lax.broadcasted_iota(jnp.int32, x.shape, 0)
    size = x.shape[0]
    up = jnp.where(rows == 0, before, pltpu.roll(x, 1, 0))
    down = jnp.where(rows == size - 1, after, pltpu.roll(x, size - 1, 0))
    return taps[0:1] * up + taps[1:2] * x + taps[2:3] * down


def product_kernel(mult, value, gate_head, gate_tail, taps_mult, taps_value, out):
    m, v = mult[...].astype(F32), value[...].astype(F32)
    product = (short(v, 0.0, 0.0, taps_value[...]) * short(m, 0.0, 0.0, taps_mult[...])).T.astype(BF16)
    zero = jnp.zeros((EDGE - 6, m.shape[1]), F32)
    heads = jnp.concatenate([v[:2], m[:2], gate_head[...].astype(F32)[:2], zero], axis=0)
    tails = jnp.concatenate([v[-2:], m[-2:], gate_tail[...].astype(F32)[-2:], zero], axis=0)
    chips, rows, width = out.shape
    part = (rows - EDGE) // CORES
    half = CORES * part
    low = lax.broadcasted_iota(jnp.int32, (EDGE, width), 1) < half
    for k in range(chips):
        at = half * k
        lane = at // width * width
        head, tail = heads[:, lane : lane + width], tails[:, lane : lane + width]
        if at == lane:
            tail = pltpu.roll(tail, half, 1)
        else:
            head = pltpu.roll(head, half, 1)
        out[k, :part, :] = product[at : at + part]
        out[k, part : part + EDGE, :] = jnp.where(low, head, tail).astype(BF16)
        out[k, part + EDGE :, :] = product[at + part : at + half]


def gains_kernel(taps_mult, taps_value, taps_gate, skip, out):
    width = out.shape[1]
    group = width // 4
    channel = (lax.axis_index(CHIP) * CORES + lax.axis_index(CORE)) * group
    lane = pl.multiple_of(channel // width * width, width)
    gains = [r[:, pl.ds(lane, width)] for r in (taps_mult, taps_value, taps_gate, skip)]
    gains = jnp.concatenate(gains + [jnp.zeros((out.shape[0] - 10, width), F32)], axis=0)
    out[...] = pltpu.roll(gains, (width - channel % width) % width, 1)


def mix_kernel(planes, other, gate, mult, value, taps_gate, taps_mult, taps_value, skip, weight, out, stage):
    core = lax.axis_index(CORE)
    chips, rows, _ = planes.shape
    group = rows // CORES
    for k in range(chips):
        near = pl.multiple_of(rows * k + core * group, group)
        far = pl.multiple_of(rows * k + (1 - core) * group, group)
        stage[pl.ds(near, group), :] = planes[k, pl.ds(pl.multiple_of(core * group, group), group), :].astype(F32)
        stage[pl.ds(far, group), :] = other[k].astype(F32)
    q = stage[...].T
    row = lax.broadcasted_iota(jnp.int32, q.shape, 0)
    border = (row == 0) | (row == q.shape[0] - 1)
    product = short(value[...].astype(F32), 0.0, 0.0, taps_value[...]) * short(mult[...].astype(F32), 0.0, 0.0, taps_mult[...])
    g = short(gate[...].astype(F32), 0.0, 0.0, taps_gate[...])
    gated = jnp.where(border, q, (q + skip[...] * product) * g).astype(BF16)
    out[...] = dot(gated, weight[...]).astype(BF16)


def filter_kernel(
    *refs, seq_len, width, chunk, group
):
    sources, out, copies, (own, stage, left_high, left_low, result, sems, out_sems) = refs[:8], refs[8], refs[9:17], refs[17:]
    channel = (lax.axis_index(CHIP) * CORES + lax.axis_index(CORE)) * group
    lane = pl.multiple_of(channel // width * width, width)
    row_at = pl.multiple_of(channel % width, group)
    sources = [x.at[:, pl.ds(lane, width)] if n in (2, 3, 4) else x for n, x in enumerate(sources)]
    moves = [pltpu.make_async_copy(a, b, sems.at[n]) for n, (a, b) in enumerate(zip(sources, copies))]
    for move in moves:
        move.start()
    for move in moves[:5]:
        move.wait()
    first, second, ahead, behind, decay, kernel_first, twist, both = copies
    hidden = second.shape[0]
    bands = (first.shape[0] - 1) // 2
    own[0] = ahead[...].T
    own[1] = behind[...].T
    own[2] = jnp.broadcast_to(decay[...], (width, width)).T
    sides = jnp.concatenate([own[0, pl.ds(row_at, group), :], own[1, pl.ds(row_at, group), :]], axis=0)
    rates = own[2, pl.ds(row_at, group), :][:, 0:1]
    rates = jnp.concatenate([rates, rates], axis=0)
    blocks = seq_len // width
    padded = 2 * bands + 8
    w1 = jnp.concatenate(
        [first[1 : 1 + 2 * bands, :], first[0:1, :], jnp.zeros((padded - 2 * bands - 1, hidden), F32)], axis=0
    )
    w1h, w1l = halves(w1 * np.float32(0.5 / math.pi))
    w1s = jnp.concatenate(
        [w1h.astype(F32), w1h.astype(F32), w1l.astype(F32), jnp.zeros((128 - 3 * padded, hidden), F32)], axis=0
    ).T.astype(BF16)
    w2h, w2l = halves(second[...].T * np.float32(0.5 / math.pi))
    w2s = jnp.concatenate([w2h, w2h, w2l], axis=1)
    w3h, w3l = halves(sides)
    w3s = jnp.concatenate([w3h, w3h, w3l], axis=1)
    row = lax.broadcasted_iota(jnp.int32, (2 * bands, chunk), 0)
    band_at = jnp.where(row < bands, row, row - bands).astype(F32)
    band = np.float32(0.0001) + band_at * np.float32((bands - 1 - 0.0001) / (bands - 1))
    band = jnp.where(row < bands, band, -band)
    offset = jnp.where(row < bands, np.float32(0.0), -QUARTER)
    head_row = lax.broadcasted_iota(jnp.int32, (8, chunk), 0)

    def step(i, total):
        at = i * chunk
        position = (lax.broadcasted_iota(jnp.int32, (1, chunk), 1) + at).astype(F32)
        tau = position / np.float32(seq_len - 1)
        trig = cosine_of_turns(position * np.float32(1.0 / seq_len) * band + offset)
        feats = jnp.concatenate([trig, jnp.where(head_row == 0, tau, 0.0)], axis=0)
        fh = feats.astype(BF16).astype(F32)
        fs = jnp.concatenate(
            [fh, feats - fh, fh, jnp.zeros((128 - 3 * padded, chunk), F32)], axis=0
        ).astype(BF16)
        h1h, h1l = halves(sine_of_turns(dot(w1s, fs)))
        h2h, h2l = halves(sine_of_turns(dot(w2s, jnp.concatenate([h1h, h1l, h1h], axis=0))))
        values = dot(w3s, jnp.concatenate([h2h, h2l, h2h], axis=0))
        values = values * jnp.exp(-rates * tau)
        side_row = lax.broadcasted_iota(jnp.int32, values.shape, 0)
        values = jnp.where((side_row >= group) & (position < 0.5), 0.0, values)
        for j in range(chunk // width):
            part = values[:, j * width : (j + 1) * width]
            total = total + part * part
            start = pl.multiple_of((i * (chunk // width) + j) * 2 * group, 2 * group)
            stage[pl.ds(start, 2 * group), :] = part
        return total

    total = lax.fori_loop(0, seq_len // chunk, step, jnp.zeros((2 * group, width), F32))
    power = jnp.sum(total, axis=1, keepdims=True)
    scale = lax.rsqrt(power[:group] + power[group:] + np.float32(1e-06))
    for move in moves[5:]:
        move.wait()
    cos, sin = twist[0], twist[1]
    cos2, sin2 = jnp.concatenate([cos, cos], axis=1), jnp.concatenate([sin, sin], axis=1)
    for c in range(group):
        x = jnp.concatenate(
            [stage[pl.ds(c, blocks, stride=2 * group), :], stage[pl.ds(group + c, blocks, stride=2 * group), :]], axis=1
        )
        xh, xl = halves(x * scale[c : c + 1, :])
        z = dot(kernel_first[...], jnp.concatenate([xh, xl, xh], axis=0))
        re, im = z[:blocks], z[blocks:]
        re, im = re * cos2 + im * sin2, im * cos2 - re * sin2
        left = jnp.concatenate([re[:, :width], im[:, :width], re[:, width:], im[:, width:]], axis=1)
        high, low = halves(left)
        left_high[c * blocks : (c + 1) * blocks, :] = high
        left_low[c * blocks : (c + 1) * blocks, :] = low
    pieces = out_sems.shape[0]
    size = group * blocks // pieces
    writes = []
    for n in range(pieces):
        part = slice(n * size, (n + 1) * size)
        high, low = left_high[part, :], left_low[part, :]
        result[part, :] = dot(high, both[0]) + dot(low, both[0]) + dot(high, both[1])
        writes.append(pltpu.make_async_copy(result.at[part, :], out.at[part, :], out_sems.at[n]))
        writes[-1].start()
    for write in writes:
        write.wait()


def conv_kernel(
    plane, partner, gains, spec, data_first, twist, ahead, back, last,
    out, stage, left_high, left_low, *, group
):
    chips, rows, width = partner.shape
    blocks = chips * CORES
    core = lax.axis_index(CORE)
    pitch = group + 2 * EDGE
    base = pl.multiple_of(EDGE * (1 - core), EDGE)
    own_at = pl.multiple_of(core * group, group)
    for k in range(chips):
        near = pl.multiple_of((CORES * k + core) * pitch + base, EDGE)
        far = pl.multiple_of((CORES * k + 1 - core) * pitch + base, EDGE)
        stage[pl.ds(near, rows), :] = plane[k, pl.ds(own_at, rows), :].astype(F32)
        stage[pl.ds(far, rows), :] = partner[k].astype(F32)

    tm, tv, tg, gain = gains[0:3], gains[3:6], gains[6:9], gains[9:10]
    edge_at = (group + EDGE) * (1 - core)
    first = [
        pltpu.roll(stage[pl.ds(edge_at + q, blocks, stride=pitch), :], (width - core * group) % width, 1) for q in range(6)
    ]
    v0, v1, m0, m1, g0, g1 = first
    v2, v3, m2, m3, g2, g3 = [pltpu.roll(x, width - CORES * group, 1) for x in first]
    row = lax.broadcasted_iota(jnp.int32, (blocks, width), 0)
    column = lax.broadcasted_iota(jnp.int32, (blocks, width), 1)

    def head(t, previous, x, following):
        return t[0:1] * jnp.where(row == 0, 0.0, pltpu.roll(previous, 1, 0)) + t[1:2] * x + t[2:3] * following

    def tail(t, previous, x, following):
        after = jnp.where(row == blocks - 1, 0.0, pltpu.roll(following, blocks - 1, 0))
        return t[0:1] * previous + t[1:2] * x + t[2:3] * after

    odd = column % 2 == 1

    def pair(heads, tails):
        tails = pltpu.roll(tails, width - 1, 1)
        return jnp.where(odd, tails, heads), jnp.where(odd, heads, tails)

    def at_ends(pairs, c):
        return pltpu.roll(pairs[c % 2], (width - c) % width, 1)

    heads = head(tv, v3, v0, v1) * head(tm, m3, m0, m1)
    tails = tail(tv, v2, v3, v0) * tail(tm, m2, m3, m0)
    edges = pair(heads, tails)
    skips = pair(gain * heads, gain * tails)
    gates = pair(head(tg, g3, g0, g1), tail(tg, g2, g3, g0))
    border = (column == 0) | (column == width - 1)

    cos, sin = twist[0], twist[1]
    for c in range(group):
        x = stage[pl.ds(EDGE + c, blocks, stride=pitch), :]
        x = jnp.where(border, at_ends(edges, c), x).astype(BF16)
        z = dot(data_first[...], jnp.concatenate([x, x], axis=0))
        re, im = z[:blocks], z[blocks:]
        left = jnp.concatenate([re * cos + im * sin, im * cos - re * sin], axis=1)
        high, low = halves(left)
        left_high[c * blocks : (c + 1) * blocks, :] = high
        left_low[c * blocks : (c + 1) * blocks, :] = low
    s = dot(left_high[...], ahead[0]) + dot(left_low[...], ahead[0]) + dot(left_high[...], ahead[1])
    sr, si = s[:, :width], s[:, width:]
    kr, ki = spec[:, :width], spec[:, width:]
    high, low = halves(jnp.concatenate([sr * kr - si * ki, sr * ki + si * kr], axis=1))
    v = dot(high, back[0]) + dot(low, back[0]) + dot(high, back[1])
    for c in range(group):
        vr = v[c * blocks : (c + 1) * blocks, :width]
        vi = v[c * blocks : (c + 1) * blocks, width:]
        high, low = halves(jnp.concatenate([vr * cos - vi * sin, vi * cos + vr * sin], axis=0))
        y = dot(last[...], jnp.concatenate([high, low, high], axis=0))
        y = jnp.where(border, (y + at_ends(skips, c)) * at_ends(gates, c), y)
        stage[pl.ds(c, blocks, stride=group), :] = y
    out[...] = stage[: blocks * group, :].astype(BF16)


def body(
    gate_in,
    mult_in,
    value_in,
    taps_gate,
    taps_mult,
    taps_value,
    filter_first,
    filter_second,
    filter_ahead,
    filter_behind,
    filter_decay,
    skip_gain,
    out_weight,
):
    chips, core = lax.axis_size(CHIP), lax.axis_index(CORE)
    cols = chips * CORES
    width, channels = gate_in.shape[1:]
    seq_len = width * cols
    group = channels // cols
    gate, mult, value = gate_in[0], mult_in[0], value_in[0]
    t = tables(cols, width)
    swap = [(i, i + 1 - 2 * (i % CORES)) for i in range(cols)]

    rows = CORES * group + EDGE
    theirs_at = ((1 - core) * group).astype(jnp.uint32)
    whole = lambda x: pl.BlockSpec(x.shape, lambda i: (0, 0))
    strip = 16
    product = pl.pallas_call(
        product_kernel,
        grid=(1,),
        in_specs=[
            whole(mult),
            whole(value),
            pl.BlockSpec((strip, channels), lambda i: (0, 0)),
            pl.BlockSpec((strip, channels), lambda i: (width // strip - 1, 0)),
            whole(taps_mult),
            whole(taps_value),
        ],
        out_specs=pl.BlockSpec((chips, rows, width), lambda i: (0, 0, 0)),
        out_shape=jax.ShapeDtypeStruct((chips, rows, width), BF16),
        compiler_params=pltpu.CompilerParams(vmem_limit_bytes=ALL_VMEM),
        name="product",
    )(mult, value, gate, gate, taps_mult, taps_value)
    plane = lax.all_to_all(product, CHIP, 0, 0, tiled=True)
    filter_args = (
        filter_first, filter_second, filter_ahead, filter_behind, filter_decay[None], t["kernel_first"], t["twist"], t["both"]
    )
    spec = pl.pallas_call(
        functools.partial(filter_kernel, seq_len=seq_len, width=width, chunk=4 * width, group=group),
        in_specs=[pl.BlockSpec(memory_space=pltpu.HBM)] * len(filter_args),
        out_specs=pl.BlockSpec(memory_space=pltpu.HBM),
        out_shape=jax.ShapeDtypeStruct((group * cols, 2 * width), F32),
        scratch_shapes=[
            pltpu.VMEM((x.shape[0], width) if n in (2, 3, 4) else x.shape, x.dtype) for n, x in enumerate(filter_args)
        ]
        + [
            pltpu.VMEM((3, width, width), F32),
            pltpu.VMEM((2 * group * cols, width), F32),
            pltpu.VMEM((group * cols, 4 * width), BF16),
            pltpu.VMEM((group * cols, 4 * width), BF16),
            pltpu.VMEM((group * cols, 2 * width), F32),
            pltpu.SemaphoreType.DMA((len(filter_args),)),
            pltpu.SemaphoreType.DMA((4,)),
        ],
        compiler_params=pltpu.CompilerParams(vmem_limit_bytes=ALL_VMEM - 320 * 1024),
        cost_estimate=cost(10, 2**22),
        name="filter",
    )(*filter_args)
    spec, taps_near, gain_near = lax.optimization_barrier((spec, (taps_mult, taps_value, taps_gate), skip_gain[None]))
    gains = pl.pallas_call(
        gains_kernel,
        out_shape=jax.ShapeDtypeStruct((16, width), F32),
        compiler_params=limit(1),
        cost_estimate=cost(20, 2**21),
        name="gains",
    )(*taps_near, gain_near)
    plane, spec, gains = lax.optimization_barrier((plane, spec, gains))
    partner = lax.ppermute(lax.dynamic_slice_in_dim(plane, theirs_at, group + EDGE, 1), COL, swap)

    convolved = pl.pallas_call(
        functools.partial(conv_kernel, group=group),
        out_shape=jax.ShapeDtypeStruct((channels, width), BF16),
        scratch_shapes=[
            pltpu.VMEM((cols * (group + 2 * EDGE), width), F32),
            pltpu.VMEM((channels, 2 * width), BF16),
            pltpu.VMEM((channels, 2 * width), BF16),
        ],
        compiler_params=limit(16),
        cost_estimate=cost(3, 2**21),
        name="conv",
    )(plane, partner, gains, spec, t["data_first"], t["twist"], t["ahead"], t["back"], t["last"])

    planes = lax.all_to_all(convolved.reshape(chips, CORES * group, width), CHIP, 0, 0, tiled=True)
    theirs = lax.dynamic_slice_in_dim(planes, theirs_at, group, 1)
    other = lax.ppermute(theirs, COL, swap)
    mixed = pl.pallas_call(
        mix_kernel,
        out_shape=jax.ShapeDtypeStruct((width, out_weight.shape[1]), BF16),
        scratch_shapes=[pltpu.VMEM((channels, width), F32)],
        compiler_params=limit(12),
        cost_estimate=cost(2, 2**22),
        name="mix",
    )(planes, other, gate, mult, value, taps_gate, taps_mult, taps_value, skip_gain[None], out_weight)
    return mixed[None]


def solution(mesh):
    shape = mesh.shape
    split = Mesh(
        mesh.devices.reshape(shape["grp"], shape["row"], shape["col"] // CORES, CORES), ("grp", "row", CHIP, CORE)
    )
    tokens = P(("grp", "row"), COL, None)
    in_specs = (tokens,) * 3 + (P(),) * 10
    return jax.shard_map(body, mesh=split, in_specs=in_specs, out_specs=tokens, check_vma=False)
```

```python
import functools
import math

import jax
import jax.numpy as jnp
import numpy as np
from jax import lax
from jax.experimental import pallas as pl
from jax.experimental.pallas import tpu as pltpu
from jax.sharding import Mesh
from jax.sharding import PartitionSpec as P

CHIP = "col_chip"
CORE = "col_core"
COL = (CHIP, CORE)
CORES = 2
EDGE = 8
ALL_VMEM = 67_000_000
F32 = jnp.float32
BF16 = jnp.bfloat16

def sine_coefficients(terms):
    nodes = np.cos((np.arange(4000) + 0.5) * math.pi / 8000) * 0.25
    basis = np.stack([nodes ** (2 * j + 1) for j in range(terms)], axis=1)
    return [np.float32(v) for v in np.linalg.lstsq(basis, np.sin(2.0 * math.pi * nodes), rcond=None)[0]]


SINE = sine_coefficients(4)
QUARTER = np.float32(0.25)


def cosine_of_turns(u):
    w = QUARTER - jnp.abs(u - jnp.round(u))
    z = w * w
    total = SINE[-1] * z + SINE[-2]
    for c in SINE[-3::-1]:
        total = total * z + c
    return total * w


def sine_of_turns(t):
    return cosine_of_turns(t - QUARTER)


def halves(x):
    high = x.astype(BF16)
    return high, (x - high.astype(F32)).astype(BF16)


def np_halves(x):
    high = np.asarray(x, np.float32).astype(BF16)
    return high, (np.asarray(x, np.float32) - high.astype(np.float32)).astype(BF16)


def cost(microseconds, size):
    return pl.CostEstimate(flops=int(microseconds * 4e8), bytes_accessed=size, transcendentals=0)


def limit(mebibytes):
    return pltpu.CompilerParams(vmem_limit_bytes=mebibytes * 2**20)


def dot(a, b):
    return jnp.dot(a, b, preferred_element_type=F32)


def tables(blocks, width):
    span = 2 * blocks * width
    freq = np.arange(blocks) + 0.5
    first = 2.0 * math.pi * np.outer(freq, np.arange(blocks)) / (2 * blocks)
    t1 = np.concatenate([np.cos(first), -np.sin(first)], axis=0)
    t3 = np.concatenate([np.cos(first).T, -np.sin(first).T], axis=1) * (2.0 / span)
    twist = 2.0 * math.pi * np.outer(freq, np.arange(width)) / span
    second = 2.0 * math.pi * (np.outer(np.arange(width), np.arange(width)) % width) / width
    c, s = np.cos(second), np.sin(second)
    ahead = np.block([[c, -s], [s, c]])
    back = np.block([[c, s], [-s, c]])
    mirror = ahead * np.where(np.arange(2 * width) < width, 1.0, -1.0)
    t1h, t1l = np_halves(t1)
    t3h, t3l = np_halves(t3)
    return {
        "data_first": np.concatenate([t1h, t1l], axis=1),
        "kernel_first": np.concatenate([t1h, t1h, t1l], axis=1),
        "last": np.concatenate([t3h, t3h, t3l], axis=1),
        "twist": np.stack([np.cos(twist), np.sin(twist)]).astype(np.float32),
        "ahead": np.stack(np_halves(ahead)),
        "both": np.stack(np_halves(np.concatenate([ahead, mirror], axis=0))),
        "back": np.stack(np_halves(back)),
    }


def short(x, before, after, taps):
    rows = lax.broadcasted_iota(jnp.int32, x.shape, 0)
    size = x.shape[0]
    up = jnp.where(rows == 0, before, pltpu.roll(x, 1, 0))
    down = jnp.where(rows == size - 1, after, pltpu.roll(x, size - 1, 0))
    return taps[0:1] * up + taps[1:2] * x + taps[2:3] * down


def product_kernel(mult, value, gate_head, gate_tail, taps_mult, taps_value, out):
    m, v = mult[...].astype(F32), value[...].astype(F32)
    product = (short(v, 0.0, 0.0, taps_value[...]) * short(m, 0.0, 0.0, taps_mult[...])).T.astype(BF16)
    zero = jnp.zeros((EDGE - 6, m.shape[1]), F32)
    heads = jnp.concatenate([v[:2], m[:2], gate_head[...].astype(F32)[:2], zero], axis=0)
    tails = jnp.concatenate([v[-2:], m[-2:], gate_tail[...].astype(F32)[-2:], zero], axis=0)
    chips, rows, width = out.shape
    part = (rows - EDGE) // CORES
    half = CORES * part
    low = lax.broadcasted_iota(jnp.int32, (EDGE, width), 1) < half
    for k in range(chips):
        at = half * k
        lane = at // width * width
        head, tail = heads[:, lane : lane + width], tails[:, lane : lane + width]
        if at == lane:
            tail = pltpu.roll(tail, half, 1)
        else:
            head = pltpu.roll(head, half, 1)
        out[k, :part, :] = product[at : at + part]
        out[k, part : part + EDGE, :] = jnp.where(low, head, tail).astype(BF16)
        out[k, part + EDGE :, :] = product[at + part : at + half]


def gains_kernel(taps_mult, taps_value, taps_gate, skip, out):
    width = out.shape[1]
    group = width // 4
    channel = (lax.axis_index(CHIP) * CORES + lax.axis_index(CORE)) * group
    lane = pl.multiple_of(channel // width * width, width)
    gains = [r[:, pl.ds(lane, width)] for r in (taps_mult, taps_value, taps_gate, skip)]
    gains = jnp.concatenate(gains + [jnp.zeros((out.shape[0] - 10, width), F32)], axis=0)
    out[...] = pltpu.roll(gains, (width - channel % width) % width, 1)


def mix_kernel(planes, other, gate, mult, value, taps_gate, taps_mult, taps_value, skip, weight, out, stage):
    core = lax.axis_index(CORE)
    chips, rows, _ = planes.shape
    group = rows // CORES
    for k in range(chips):
        near = pl.multiple_of(rows * k + core * group, group)
        far = pl.multiple_of(rows * k + (1 - core) * group, group)
        stage[pl.ds(near, group), :] = planes[k, pl.ds(pl.multiple_of(core * group, group), group), :].astype(F32)
        stage[pl.ds(far, group), :] = other[k].astype(F32)
    q = stage[...].T
    row = lax.broadcasted_iota(jnp.int32, q.shape, 0)
    border = (row == 0) | (row == q.shape[0] - 1)
    product = short(value[...].astype(F32), 0.0, 0.0, taps_value[...]) * short(mult[...].astype(F32), 0.0, 0.0, taps_mult[...])
    g = short(gate[...].astype(F32), 0.0, 0.0, taps_gate[...])
    gated = jnp.where(border, q, (q + skip[...] * product) * g).astype(BF16)
    out[...] = dot(gated, weight[...]).astype(BF16)


def filter_kernel(
    *refs, seq_len, width, chunk, group
):
    sources, out, copies, (own, stage, left_high, left_low, result, sems, out_sems) = refs[:8], refs[8], refs[9:17], refs[17:]
    channel = (lax.axis_index(CHIP) * CORES + lax.axis_index(CORE)) * group
    lane = pl.multiple_of(channel // width * width, width)
    row_at = pl.multiple_of(channel % width, group)
    sources = [x.at[:, pl.ds(lane, width)] if n in (2, 3, 4) else x for n, x in enumerate(sources)]
    moves = [pltpu.make_async_copy(a, b, sems.at[n]) for n, (a, b) in enumerate(zip(sources, copies))]
    for move in moves:
        move.start()
    for move in moves[:5]:
        move.wait()
    first, second, ahead, behind, decay, kernel_first, twist, both = copies
    hidden = second.shape[0]
    bands = (first.shape[0] - 1) // 2
    own[0] = ahead[...].T
    own[1] = behind[...].T
    own[2] = jnp.broadcast_to(decay[...], (width, width)).T
    sides = jnp.concatenate([own[0, pl.ds(row_at, group), :], own[1, pl.ds(row_at, group), :]], axis=0)
    rates = own[2, pl.ds(row_at, group), :][:, 0:1]
    rates = jnp.concatenate([rates, rates], axis=0)
    blocks = seq_len // width
    padded = 2 * bands + 8
    w1 = jnp.concatenate(
        [first[1 : 1 + 2 * bands, :], first[0:1, :], jnp.zeros((padded - 2 * bands - 1, hidden), F32)], axis=0
    )
    w1h, w1l = halves(w1 * np.float32(0.5 / math.pi))
    w1s = jnp.concatenate(
        [w1h.astype(F32), w1h.astype(F32), w1l.astype(F32), jnp.zeros((128 - 3 * padded, hidden), F32)], axis=0
    ).T.astype(BF16)
    w2h, w2l = halves(second[...].T * np.float32(0.5 / math.pi))
    w2s = jnp.concatenate([w2h, w2h, w2l], axis=1)
    w3h, w3l = halves(sides)
    w3s = jnp.concatenate([w3h, w3h, w3l], axis=1)
    row = lax.broadcasted_iota(jnp.int32, (2 * bands, chunk), 0)
    band_at = jnp.where(row < bands, row, row - bands).astype(F32)
    band = np.float32(0.0001) + band_at * np.float32((bands - 1 - 0.0001) / (bands - 1))
    band = jnp.where(row < bands, band, -band)
    offset = jnp.where(row < bands, np.float32(0.0), -QUARTER)
    head_row = lax.broadcasted_iota(jnp.int32, (8, chunk), 0)

    def step(i, total):
        at = i * chunk
        position = (lax.broadcasted_iota(jnp.int32, (1, chunk), 1) + at).astype(F32)
        tau = position / np.float32(seq_len - 1)
        trig = cosine_of_turns(position * np.float32(1.0 / seq_len) * band + offset)
        feats = jnp.concatenate([trig, jnp.where(head_row == 0, tau, 0.0)], axis=0)
        fh = feats.astype(BF16).astype(F32)
        fs = jnp.concatenate(
            [fh, feats - fh, fh, jnp.zeros((128 - 3 * padded, chunk), F32)], axis=0
        ).astype(BF16)
        h1h, h1l = halves(sine_of_turns(dot(w1s, fs)))
        h2h, h2l = halves(sine_of_turns(dot(w2s, jnp.concatenate([h1h, h1l, h1h], axis=0))))
        values = dot(w3s, jnp.concatenate([h2h, h2l, h2h], axis=0))
        values = values * jnp.exp(-rates * tau)
        side_row = lax.broadcasted_iota(jnp.int32, values.shape, 0)
        values = jnp.where((side_row >= group) & (position < 0.5), 0.0, values)
        for j in range(chunk // width):
            part = values[:, j * width : (j + 1) * width]
            total = total + part * part
            start = pl.multiple_of((i * (chunk // width) + j) * 2 * group, 2 * group)
            stage[pl.ds(start, 2 * group), :] = part
        return total

    total = lax.fori_loop(0, seq_len // chunk, step, jnp.zeros((2 * group, width), F32))
    power = jnp.sum(total, axis=1, keepdims=True)
    scale = lax.rsqrt(power[:group] + power[group:] + np.float32(1e-06))
    for move in moves[5:]:
        move.wait()
    cos, sin = twist[0], twist[1]
    cos2, sin2 = jnp.concatenate([cos, cos], axis=1), jnp.concatenate([sin, sin], axis=1)
    for c in range(group):
        x = jnp.concatenate(
            [stage[pl.ds(c, blocks, stride=2 * group), :], stage[pl.ds(group + c, blocks, stride=2 * group), :]], axis=1
        )
        xh, xl = halves(x * scale[c : c + 1, :])
        z = dot(kernel_first[...], jnp.concatenate([xh, xl, xh], axis=0))
        re, im = z[:blocks], z[blocks:]
        re, im = re * cos2 + im * sin2, im * cos2 - re * sin2
        left = jnp.concatenate([re[:, :width], im[:, :width], re[:, width:], im[:, width:]], axis=1)
        high, low = halves(left)
        left_high[c * blocks : (c + 1) * blocks, :] = high
        left_low[c * blocks : (c + 1) * blocks, :] = low
    pieces = out_sems.shape[0]
    size = group * blocks // pieces
    writes = []
    for n in range(pieces):
        part = slice(n * size, (n + 1) * size)
        high, low = left_high[part, :], left_low[part, :]
        result[part, :] = dot(high, both[0]) + dot(low, both[0]) + dot(high, both[1])
        writes.append(pltpu.make_async_copy(result.at[part, :], out.at[part, :], out_sems.at[n]))
        writes[-1].start()
    for write in writes:
        write.wait()


def conv_kernel(
    plane, partner, gains, spec, data_first, twist, ahead, back, last,
    out, stage, left_high, left_low, *, group
):
    chips, rows, width = partner.shape
    blocks = chips * CORES
    core = lax.axis_index(CORE)
    pitch = group + 2 * EDGE
    base = pl.multiple_of(EDGE * (1 - core), EDGE)
    own_at = pl.multiple_of(core * group, group)
    for k in range(chips):
        near = pl.multiple_of((CORES * k + core) * pitch + base, EDGE)
        far = pl.multiple_of((CORES * k + 1 - core) * pitch + base, EDGE)
        stage[pl.ds(near, rows), :] = plane[k, pl.ds(own_at, rows), :].astype(F32)
        stage[pl.ds(far, rows), :] = partner[k].astype(F32)

    tm, tv, tg, gain = gains[0:3], gains[3:6], gains[6:9], gains[9:10]
    edge_at = (group + EDGE) * (1 - core)
    first = [
        pltpu.roll(stage[pl.ds(edge_at + q, blocks, stride=pitch), :], (width - core * group) % width, 1) for q in range(6)
    ]
    v0, v1, m0, m1, g0, g1 = first
    v2, v3, m2, m3, g2, g3 = [pltpu.roll(x, width - CORES * group, 1) for x in first]
    row = lax.broadcasted_iota(jnp.int32, (blocks, width), 0)
    column = lax.broadcasted_iota(jnp.int32, (blocks, width), 1)

    def head(t, previous, x, following):
        return t[0:1] * jnp.where(row == 0, 0.0, pltpu.roll(previous, 1, 0)) + t[1:2] * x + t[2:3] * following

    def tail(t, previous, x, following):
        after = jnp.where(row == blocks - 1, 0.0, pltpu.roll(following, blocks - 1, 0))
        return t[0:1] * previous + t[1:2] * x + t[2:3] * after

    odd = column % 2 == 1

    def pair(heads, tails):
        tails = pltpu.roll(tails, width - 1, 1)
        return jnp.where(odd, tails, heads), jnp.where(odd, heads, tails)

    def at_ends(pairs, c):
        return pltpu.roll(pairs[c % 2], (width - c) % width, 1)

    heads = head(tv, v3, v0, v1) * head(tm, m3, m0, m1)
    tails = tail(tv, v2, v3, v0) * tail(tm, m2, m3, m0)
    edges = pair(heads, tails)
    skips = pair(gain * heads, gain * tails)
    gates = pair(head(tg, g3, g0, g1), tail(tg, g2, g3, g0))
    border = (column == 0) | (column == width - 1)

    cos, sin = twist[0], twist[1]
    for c in range(group):
        x = stage[pl.ds(EDGE + c, blocks, stride=pitch), :]
        x = jnp.where(border, at_ends(edges, c), x).astype(BF16)
        z = dot(data_first[...], jnp.concatenate([x, x], axis=0))
        re, im = z[:blocks], z[blocks:]
        left = jnp.concatenate([re * cos + im * sin, im * cos - re * sin], axis=1)
        high, low = halves(left)
        left_high[c * blocks : (c + 1) * blocks, :] = high
        left_low[c * blocks : (c + 1) * blocks, :] = low
    s = dot(left_high[...], ahead[0]) + dot(left_low[...], ahead[0]) + dot(left_high[...], ahead[1])
    sr, si = s[:, :width], s[:, width:]
    kr, ki = spec[:, :width], spec[:, width:]
    high, low = halves(jnp.concatenate([sr * kr - si * ki, sr * ki + si * kr], axis=1))
    v = dot(high, back[0]) + dot(low, back[0]) + dot(high, back[1])
    for c in range(group):
        vr = v[c * blocks : (c + 1) * blocks, :width]
        vi = v[c * blocks : (c + 1) * blocks, width:]
        high, low = halves(jnp.concatenate([vr * cos - vi * sin, vi * cos + vr * sin], axis=0))
        y = dot(last[...], jnp.concatenate([high, low, high], axis=0))
        y = jnp.where(border, (y + at_ends(skips, c)) * at_ends(gates, c), y)
        stage[pl.ds(c, blocks, stride=group), :] = y
    out[...] = stage[: blocks * group, :].astype(BF16)


def body(
    gate_in,
    mult_in,
    value_in,
    taps_gate,
    taps_mult,
    taps_value,
    filter_first,
    filter_second,
    filter_ahead,
    filter_behind,
    filter_decay,
    skip_gain,
    out_weight,
):
    chips, core = lax.axis_size(CHIP), lax.axis_index(CORE)
    cols = chips * CORES
    width, channels = gate_in.shape[1:]
    seq_len = width * cols
    group = channels // cols
    gate, mult, value = gate_in[0], mult_in[0], value_in[0]
    t = tables(cols, width)
    swap = [(i, i + 1 - 2 * (i % CORES)) for i in range(cols)]

    rows = CORES * group + EDGE
    theirs_at = ((1 - core) * group).astype(jnp.uint32)
    whole = lambda x: pl.BlockSpec(x.shape, lambda i: (0, 0))
    strip = 16
    product = pl.pallas_call(
        product_kernel,
        grid=(1,),
        in_specs=[
            whole(mult),
            whole(value),
            pl.BlockSpec((strip, channels), lambda i: (0, 0)),
            pl.BlockSpec((strip, channels), lambda i: (width // strip - 1, 0)),
            whole(taps_mult),
            whole(taps_value),
        ],
        out_specs=pl.BlockSpec((chips, rows, width), lambda i: (0, 0, 0)),
        out_shape=jax.ShapeDtypeStruct((chips, rows, width), BF16),
        compiler_params=pltpu.CompilerParams(vmem_limit_bytes=ALL_VMEM),
        name="product",
    )(mult, value, gate, gate, taps_mult, taps_value)
    plane = lax.all_to_all(product, CHIP, 0, 0, tiled=True)
    filter_args = (
        filter_first, filter_second, filter_ahead, filter_behind, filter_decay[None], t["kernel_first"], t["twist"], t["both"]
    )
    spec = pl.pallas_call(
        functools.partial(filter_kernel, seq_len=seq_len, width=width, chunk=16 * width, group=group),
        in_specs=[pl.BlockSpec(memory_space=pltpu.HBM)] * len(filter_args),
        out_specs=pl.BlockSpec(memory_space=pltpu.HBM),
        out_shape=jax.ShapeDtypeStruct((group * cols, 2 * width), F32),
        scratch_shapes=[
            pltpu.VMEM((x.shape[0], width) if n in (2, 3, 4) else x.shape, x.dtype) for n, x in enumerate(filter_args)
        ]
        + [
            pltpu.VMEM((3, width, width), F32),
            pltpu.VMEM((2 * group * cols, width), F32),
            pltpu.VMEM((group * cols, 4 * width), BF16),
            pltpu.VMEM((group * cols, 4 * width), BF16),
            pltpu.VMEM((group * cols, 2 * width), F32),
            pltpu.SemaphoreType.DMA((len(filter_args),)),
            pltpu.SemaphoreType.DMA((4,)),
        ],
        compiler_params=pltpu.CompilerParams(vmem_limit_bytes=ALL_VMEM - 320 * 1024),
        cost_estimate=cost(10, 2**22),
        name="filter",
    )(*filter_args)
    spec, taps_near, gain_near = lax.optimization_barrier((spec, (taps_mult, taps_value, taps_gate), skip_gain[None]))
    gains = pl.pallas_call(
        gains_kernel,
        out_shape=jax.ShapeDtypeStruct((16, width), F32),
        compiler_params=limit(1),
        cost_estimate=cost(20, 2**21),
        name="gains",
    )(*taps_near, gain_near)
    plane, spec, gains = lax.optimization_barrier((plane, spec, gains))
    partner = lax.ppermute(lax.dynamic_slice_in_dim(plane, theirs_at, group + EDGE, 1), COL, swap)

    convolved = pl.pallas_call(
        functools.partial(conv_kernel, group=group),
        out_shape=jax.ShapeDtypeStruct((channels, width), BF16),
        scratch_shapes=[
            pltpu.VMEM((cols * (group + 2 * EDGE), width), F32),
            pltpu.VMEM((channels, 2 * width), BF16),
            pltpu.VMEM((channels, 2 * width), BF16),
        ],
        compiler_params=limit(16),
        cost_estimate=cost(3, 2**21),
        name="conv",
    )(plane, partner, gains, spec, t["data_first"], t["twist"], t["ahead"], t["back"], t["last"])

    planes = lax.all_to_all(convolved.reshape(chips, CORES * group, width), CHIP, 0, 0, tiled=True)
    theirs = lax.dynamic_slice_in_dim(planes, theirs_at, group, 1)
    other = lax.ppermute(theirs, COL, swap)
    mixed = pl.pallas_call(
        mix_kernel,
        out_shape=jax.ShapeDtypeStruct((width, out_weight.shape[1]), BF16),
        scratch_shapes=[pltpu.VMEM((channels, width), F32)],
        compiler_params=limit(12),
        cost_estimate=cost(2, 2**22),
        name="mix",
    )(planes, other, gate, mult, value, taps_gate, taps_mult, taps_value, skip_gain[None], out_weight)
    return mixed[None]


def solution(mesh):
    shape = mesh.shape
    split = Mesh(
        mesh.devices.reshape(shape["grp"], shape["row"], shape["col"] // CORES, CORES), ("grp", "row", CHIP, CORE)
    )
    tokens = P(("grp", "row"), COL, None)
    in_specs = (tokens,) * 3 + (P(),) * 10
    return jax.shard_map(body, mesh=split, in_specs=in_specs, out_specs=tokens, check_vma=False)
```
